512 devices in a mesh: sp: 128 (over z, y, core), tp: 4 (over x).
Axes of the slice: x: 4, y: 8, z: 8, core: 2. Of those that a mesh axis runs over, the one named last changes fastest.
Arguments:
- tokens: bfloat16 [16384, 2048], P(('sp', 'tp')), may hold values from -6 to 6
- norm_gain: float32 [2048], replicated, may hold values from 0.1 to 1.9
- w_query: bfloat16 [2048, 1024], P(None, 'tp'), may hold values from -3 to 3
- w_key: bfloat16 [2048, 1024], P(None, 'tp'), may hold values from -0.15625 to 0.15625
- w_value: bfloat16 [2048, 1024], P(None, 'tp'), may hold values from -0.125 to 0.125
- w_state_in: bfloat16 [2048, 512], P(None, 'tp'), may hold values from -0.125 to 0.125
- decay_rate: float32 [32, 64], P('tp'), may hold values from 0 to 0.04, as said below
- rotation: float32 [32, 64], P('tp'), may hold values from -0.5 to 0.5
- extra_decay: float32 [16384, 32], P('sp', 'tp'), may hold values from -1 to 0, as said below
- in_map: float32 [2, 32, 64, 16], P(None, 'tp'), may hold values from -1 to 1
- out_map: float32 [2, 32, 16, 64], P(None, 'tp'), may hold values from -0.5 to 0.5
- skip_gain: float32 [32, 16], P('tp'), may hold values from -4 to 4
- init_state: float32 [8, 2, 32, 64], P(None, None, 'tp'), may hold values from -6 to 6
- mix_lambda: float32 [8], P('tp'), may hold values from 0.3 to 0.8
- sub_gain: float32 [128], replicated, may hold values from 0.1 to 1.9
- w_out_state: bfloat16 [512, 2048], P('tp', 'sp'), may hold values from -0.375 to 0.375
- w_out_attn: bfloat16 [1024, 2048], P('tp', 'sp'), may hold values from -0.1875 to 0.1875
Outputs:
- mixed_out: bfloat16 [16384, 2048], P(('sp', 'tp'))
The draws below stay inside these ranges and needn't reach their ends.
Inputs may be any that keep to these rules, and one draw needn't show every extreme that they name: `decay_rate`: positive. `extra_decay`: never positive.
All inputs are finite; a program needn't handle non-finite values.
Results may differ from the reference program's by a relative error of at most 0.017.
The reference program's roundings to bfloat16 on the way count: a program that leaves them out, or rounds other values in their place, can miss the bound.
Values may be sent and summed in bfloat16 or wider, within the bound.
No kernel may reach another device: no remote copies, remote signals or barrier semaphores. Data moves between devices by JAX's collectives and lax.ppermute only.
A program may use at most 128 MiB of HBM per device.

```python
import math
import jax
import jax.numpy as jnp
from jax import lax

D = 2048
S5_STATE_GROUPS = 32
S5_GROUP = 16
S5_STATE = 64
C_HEADS = 8
QK_DIM = 64
V_DIM = 128
SEGMENT = 64
TOK_DEV = 128
SEQS = 8
S5_WIDTH = 512
C_WIDTH = 1024
TOKEN_TOTAL = 16384
SEQUENCE_LENGTH = 2048
N_TP = 4


def draw_w_query(key, part):
    normal_values = jnp.clip(jax.random.normal(key, (D, 2 * C_HEADS * QK_DIM), jnp.float32), -6.0, 6.0)
    weight_scale = 1.3 / math.sqrt(D)
    return jnp.clip(normal_values * weight_scale, -3.0, 3.0).astype(jnp.bfloat16)


def draw_decay_rate(key, part):
    coin_key, slow_key, fast_key, spread_key = jax.random.split(key, 4)
    slow_share = 0.5
    slow_group = jax.random.uniform(coin_key, (S5_STATE_GROUPS, 1), jnp.float32) < slow_share
    slow_rate = jnp.exp(jax.random.uniform(slow_key, (S5_STATE_GROUPS, 1), jnp.float32, math.log(0.05), math.log(0.3))) / SEQUENCE_LENGTH
    fast_rate = jnp.exp(jax.random.uniform(fast_key, (S5_STATE_GROUPS, 1), jnp.float32, math.log(0.01), math.log(0.03)))
    spread_factor = jnp.exp(jax.random.uniform(spread_key, (S5_STATE_GROUPS, S5_STATE), jnp.float32, -0.2, 0.2))
    return jnp.where(slow_group, slow_rate, fast_rate) * spread_factor


def draw_extra_decay(key, part):
    factor_key, location_key, depth_random_key = jax.random.split(key, 3)
    block_total = TOKEN_TOTAL // TOK_DEV
    block_factor = jnp.exp(jax.random.uniform(factor_key, (block_total, 1, S5_STATE_GROUPS), jnp.float32, math.log(0.5), math.log(2.5)))
    constant_portion = jnp.broadcast_to(block_factor, (block_total, TOK_DEV, S5_STATE_GROUPS)).reshape(TOKEN_TOTAL, S5_STATE_GROUPS) * (-0.3 / SEQUENCE_LENGTH)
    sudden_location = jax.random.uniform(location_key, (TOKEN_TOTAL, S5_STATE_GROUPS), jnp.float32) < 2.0 / SEQUENCE_LENGTH
    sudden_depth = jnp.log(jax.random.uniform(depth_random_key, (TOKEN_TOTAL, S5_STATE_GROUPS), jnp.float32, 0.5, 0.8))
    return jnp.where(sudden_location, sudden_depth, 0.0) + constant_portion


def shard_levels(own_key, dims, cuts, least, high):
    factor_of, own = 1.0, jax.random.fold_in(own_key, 6)
    for axis_at, blocks in cuts:
        heights = jnp.exp(jax.random.uniform(jax.random.fold_in(own, axis_at), (blocks,), jnp.float32, least / len(cuts), high / len(cuts)))
        factor_of = factor_of * jnp.repeat(heights, dims[axis_at] // blocks).reshape([-1 if axis == axis_at else 1 for axis in range(len(dims))])
    return factor_of


def centred(rng, extent, deviation, bound, pieces=(), kind=jnp.bfloat16):
    drawn = deviation * jax.random.normal(rng, extent, jnp.float32)
    if pieces:
        drawn = drawn * shard_levels(rng, extent, pieces, -0.22, 0.18)
    return jnp.clip(drawn, -bound, bound).astype(kind)


def setup_inputs(seed: int = 0) -> dict:
    streams_of = jax.random.split(jax.random.key(seed), 18)
    return {
        "tokens": centred(streams_of[0], (TOKEN_TOTAL, D), 1.0, 6.0, ((0, 512),)),
        "norm_gain": jnp.clip(1.0 + 0.18 * jax.random.normal(streams_of[1], (D,), jnp.float32), 0.1, 1.9),
        "w_query": draw_w_query(jax.random.fold_in(streams_of[17], 71), 0),
        "w_key": centred(streams_of[3], (D, 2 * C_HEADS * QK_DIM), (3 * D // 5) ** -0.5, 0.15625, ((1, 4),)),
        "w_value": centred(streams_of[4], (D, C_WIDTH), D ** -0.5, 0.125, ((1, 4),)),
        "w_state_in": centred(streams_of[5], (D, S5_WIDTH), D ** -0.5, 0.125, ((1, 4),)),
        "decay_rate": draw_decay_rate(jax.random.fold_in(streams_of[17], 71), 0),
        "rotation": jnp.clip(jax.random.uniform(streams_of[7], (S5_STATE_GROUPS, S5_STATE), jnp.float32, -0.5, 0.5) * shard_levels(streams_of[7], (S5_STATE_GROUPS, S5_STATE), ((0, 4),), -0.4, 0.0), -0.5, 0.5),
        "extra_decay": draw_extra_decay(jax.random.fold_in(streams_of[17], 71), 0),
        "in_map": centred(streams_of[9], (2, S5_STATE_GROUPS, S5_STATE, S5_GROUP), (2 * S5_GROUP) ** -0.5, 1.0, ((1, 4),), jnp.float32),
        "out_map": centred(streams_of[10], (2, S5_STATE_GROUPS, S5_GROUP, S5_STATE), (2 * S5_STATE) ** -0.5, 0.5, ((1, 4),), jnp.float32),
        "skip_gain": centred(streams_of[11], (S5_STATE_GROUPS, S5_GROUP), 1.0, 4.0, ((0, 4),), jnp.float32),
        "init_state": centred(streams_of[12], (SEQS, 2, S5_STATE_GROUPS, S5_STATE), 1.5, 6.0, ((2, 4),), jnp.float32),
        "mix_lambda": jnp.clip(0.3 + 0.5 * jax.random.uniform(streams_of[13], (C_HEADS,), jnp.float32) ** shard_levels(streams_of[13], (C_HEADS,), ((0, 4),), -0.2, 0.2), 0.3, 0.8),
        "sub_gain": jnp.clip(1.0 + 0.18 * jax.random.normal(streams_of[14], (V_DIM,), jnp.float32), 0.1, 1.9),
        "w_out_state": centred(streams_of[15], (S5_WIDTH, D), (S5_WIDTH // 2) ** -0.5, 0.375, ((0, 4), (1, 128))),
        "w_out_attn": centred(streams_of[16], (C_WIDTH, D), C_WIDTH ** -0.5, 0.1875, ((0, 4), (1, 128))),
    }


EPSILON = 1e-06
ROTARY_BASE = 10000.0
LAMBDA_INIT = 0.2
MASK_FLOOR = -1e+30

def rotary(values, positions):
    half_width = values.shape[-1] // 2
    inverse = ROTARY_BASE ** (-2.0 * jnp.arange(half_width, dtype=jnp.float32) / values.shape[-1])
    angles = positions.astype(jnp.float32)[:, None] * inverse[None, :]
    cosine_table = jnp.cos(angles)[:, None, :]
    sine_table = jnp.sin(angles)[:, None, :]
    first_half = values[..., :half_width]
    second_half = values[..., half_width:]
    return jnp.concatenate((first_half * cosine_table - second_half * sine_table, first_half * sine_table + second_half * cosine_table), axis=-1)

def chain_combine(earlier, later):
    early_mult_real, early_mult_imag, early_add_real, early_add_imag = earlier
    late_mult_real, late_mult_imag, late_add_real, late_add_imag = later
    return (late_mult_real * early_mult_real - late_mult_imag * early_mult_imag, late_mult_real * early_mult_imag + late_mult_imag * early_mult_real, late_mult_real * early_add_real - late_mult_imag * early_add_imag + late_add_real, late_mult_real * early_add_imag + late_mult_imag * early_add_real + late_add_imag)

def take_sequence(values, sequence):
    blocks = values.reshape((-1, SEQS, TOK_DEV) + values.shape[1:])
    return blocks[:, sequence].reshape((-1,) + values.shape[1:])

def lay_back(parts):
    shaped = [part.reshape((-1, TOK_DEV) + part.shape[1:]) for part in parts]
    stacked = jnp.stack(shaped, axis=1)
    return stacked.reshape((TOKEN_TOTAL,) + parts[0].shape[1:])

def attention(query_heads, key_heads, value_heads, mix_lambda, sub_gain):
    seq_length = query_heads.shape[0]
    block_rows = math.gcd(seq_length, 1024)
    segment_ids = jnp.arange(seq_length, dtype=jnp.int32) // SEGMENT
    outputs = []
    for first_row in range(0, seq_length, block_rows):
        stop_row = first_row + block_rows
        query_block = query_heads[first_row:stop_row].astype(jnp.float32)
        key_block = key_heads[:stop_row].astype(jnp.float32)
        scores = jnp.einsum('qhcd,khcd->hcqk', query_block, key_block) * QK_DIM ** (-0.5)
        allowed = segment_ids[:stop_row][None, :] <= segment_ids[first_row:stop_row][:, None]
        masked = jnp.where(allowed, scores, MASK_FLOOR)
        row_peak = lax.optimization_barrier(jnp.max(masked, axis=-1, keepdims=True))
        exponent = jnp.where(allowed, jnp.exp(masked - row_peak), 0.0)
        totals = lax.optimization_barrier(jnp.sum(exponent, axis=-1))
        rounded = lax.optimization_barrier(exponent.astype(jnp.bfloat16)).astype(jnp.float32)
        numerators = jnp.einsum('hcqk,khd->hcqd', rounded, value_heads[:stop_row].astype(jnp.float32))
        difference = numerators[:, 0] / totals[:, 0, :, None] - mix_lambda[:, None, None] * numerators[:, 1] / totals[:, 1, :, None]
        difference = jnp.transpose(difference, (1, 0, 2))
        normed_heads = difference * lax.rsqrt(lax.optimization_barrier(jnp.mean(difference * difference, axis=-1, keepdims=True)) + EPSILON) * sub_gain * (1.0 - LAMBDA_INIT)
        outputs.append(normed_heads.astype(jnp.bfloat16).reshape(block_rows, -1))
    return jnp.concatenate(outputs, axis=0)

def state_mixer(state_drive, decay_rate, rotation, extra_decay, in_map, out_map, skip_gain, start_state):
    highest = lax.Precision.HIGHEST
    step_count, group_count = extra_decay.shape
    drive_wide = state_drive.astype(jnp.float32).reshape(step_count, group_count, -1)
    magnitude = jnp.exp(extra_decay[:, :, None] - decay_rate[None])
    trans_real = magnitude * jnp.cos(rotation)[None]
    trans_imag = magnitude * jnp.sin(rotation)[None]
    in_scale = jnp.sqrt(-jnp.expm1(-2.0 * decay_rate))
    inject_real = in_scale * jnp.einsum('gnp,tgp->tgn', in_map[0], drive_wide, precision=highest)
    inject_imag = in_scale * jnp.einsum('gnp,tgp->tgn', in_map[1], drive_wide, precision=highest)
    mult_real, mult_imag, add_real, add_imag = lax.associative_scan(chain_combine, (trans_real, trans_imag, inject_real, inject_imag), axis=0)
    state_real = mult_real * start_state[0] - mult_imag * start_state[1] + add_real
    state_imag = mult_real * start_state[1] + mult_imag * start_state[0] + add_imag
    mixed_state = jnp.einsum('gpn,tgn->tgp', out_map[0], state_real, precision=highest) - jnp.einsum('gpn,tgn->tgp', out_map[1], state_imag, precision=highest) + skip_gain * drive_wide
    return jax.nn.gelu(mixed_state).astype(jnp.bfloat16).reshape(step_count, -1)

def reference(tokens, norm_gain, w_query, w_key, w_value, w_state_in, decay_rate, rotation, extra_decay, in_map, out_map, skip_gain, init_state, mix_lambda, sub_gain, w_out_state, w_out_attn):
    tokens_wide = tokens.astype(jnp.float32)
    normed = (tokens_wide * lax.rsqrt(lax.optimization_barrier(jnp.mean(tokens_wide * tokens_wide, axis=-1, keepdims=True)) + EPSILON) * norm_gain).astype(jnp.bfloat16)
    token_ids = jnp.arange(TOKEN_TOTAL, dtype=jnp.int32)
    positions = token_ids // TOK_DEV // SEQS * TOK_DEV + token_ids % TOK_DEV
    query_raw = jnp.dot(normed, w_query, preferred_element_type=jnp.float32).reshape(TOKEN_TOTAL, 2 * C_HEADS, QK_DIM)
    query_heads = rotary(query_raw, positions).astype(jnp.bfloat16).reshape(TOKEN_TOTAL, C_HEADS, 2, QK_DIM)
    key_raw = jnp.dot(normed, w_key, preferred_element_type=jnp.float32).reshape(TOKEN_TOTAL, 2 * C_HEADS, QK_DIM)
    key_heads = rotary(key_raw, positions).astype(jnp.bfloat16).reshape(TOKEN_TOTAL, C_HEADS, 2, QK_DIM)
    value_heads = jnp.dot(normed, w_value, preferred_element_type=jnp.float32).astype(jnp.bfloat16).reshape(TOKEN_TOTAL, C_HEADS, V_DIM)
    state_drive = jnp.dot(normed, w_state_in, preferred_element_type=jnp.float32).astype(jnp.bfloat16)
    attn_parts = []
    state_parts = []
    for sequence in range(SEQS):
        attn_parts.append(attention(take_sequence(query_heads, sequence), take_sequence(key_heads, sequence), take_sequence(value_heads, sequence), mix_lambda, sub_gain))
        state_parts.append(state_mixer(take_sequence(state_drive, sequence), decay_rate, rotation, take_sequence(extra_decay, sequence), in_map, out_map, skip_gain, init_state[sequence]))
    attn_out = lay_back(attn_parts)
    state_out = lay_back(state_parts)
    state_share = S5_WIDTH // N_TP
    attn_share = C_WIDTH // N_TP
    summed = jnp.zeros((TOKEN_TOTAL, D), jnp.float32)
    for head_part in range(N_TP):
        state_cols = state_out[:, head_part * state_share:(head_part + 1) * state_share]
        attn_cols = attn_out[:, head_part * attn_share:(head_part + 1) * attn_share]
        partial_sum = jnp.dot(state_cols, w_out_state[head_part * state_share:(head_part + 1) * state_share], preferred_element_type=jnp.float32) + jnp.dot(attn_cols, w_out_attn[head_part * attn_share:(head_part + 1) * attn_share], preferred_element_type=jnp.float32)
        summed = summed + lax.optimization_barrier(partial_sum.astype(jnp.bfloat16)).astype(jnp.float32)
    return summed.astype(jnp.bfloat16)
```

```python
import jax
import jax.numpy as jnp
from jax import lax
from jax.experimental import pallas as pl
from jax.experimental.pallas import tpu as pltpu
from jax.sharding import Mesh
from jax.sharding import PartitionSpec as P

SP = ("z", "h", "q", "c")
SP_TP = ("z", "h", "q", "c", "tp")

EPSILON = 1e-06
ROTARY_BASE = 10000.0
LAMBDA_INIT = 0.2
MASK_FLOOR = -1e30
ROWS = 128
SUBS = 8
STEPS = ROWS // SUBS
LANES = 128
QK_DIM = 64
SEGMENT = 64
STATE_WIDTH = 512
GROUPS = 8
GROUP = 16
STATES = 64
EL_ROWS = 16
RING = 8


f32 = jnp.float32
bf16 = jnp.bfloat16


def dot(a, b):
    return jnp.dot(a, b, preferred_element_type=f32)


def dot_nt(a, b):
    return lax.dot_general(a, b, (((1,), (1,)), ((), ())), preferred_element_type=f32)


def split_two(x):
    high = x.astype(bf16)
    return high, (x - high.astype(f32)).astype(bf16)


def row_order(transposed):
    first = lax.broadcasted_iota(jnp.int32, (ROWS, ROWS), 0)
    second = lax.broadcasted_iota(jnp.int32, (ROWS, ROWS), 1)
    row, token = (second, first) if transposed else (first, second)
    return (row % SUBS) * STEPS + row // SUBS == token


def transitions_kernel(extra, decay, cosine, sine, a_re, a_im, m_re, m_im):
    group = lax.broadcasted_iota(jnp.int32, (GROUPS, STATE_WIDTH), 0)
    lane = lax.broadcasted_iota(jnp.int32, (GROUPS, STATE_WIDTH), 1)
    widen = (lane // STATES == group).astype(f32)
    highest = lax.Precision.HIGHEST
    ordered = jnp.dot(
        row_order(False).astype(f32), extra[...], precision=highest, preferred_element_type=f32
    )
    wide = jnp.dot(ordered, widen, precision=highest, preferred_element_type=f32)
    magnitude = jnp.exp(wide - decay[...])
    real, imag = magnitude * cosine[...], magnitude * sine[...]
    a_re[...] = real
    a_im[...] = imag
    run_re, run_im = real[:SUBS], imag[:SUBS]
    m_re[:SUBS, :] = run_re
    m_im[:SUBS, :] = run_im
    for step in range(1, STEPS):
        rows = slice(step * SUBS, (step + 1) * SUBS)
        tr, ti = real[rows], imag[rows]
        run_re, run_im = tr * run_re - ti * run_im, tr * run_im + ti * run_re
        m_re[rows, :] = run_re
        m_im[rows, :] = run_im


def project_kernel(
    place,
    tokens,
    gain,
    w_query,
    w_key,
    w_value,
    w_state,
    cosine,
    sine,
    in_high,
    in_low,
    a_re,
    a_im,
    m_re,
    m_im,
    keep,
    send,
    s_re,
    s_im,
    x_re,
    x_im,
    drive_out,
):
    head = place[1]
    wide = tokens[...].astype(f32)
    scale = lax.rsqrt(jnp.mean(wide * wide, axis=-1, keepdims=True) + EPSILON)
    normed = (wide * scale * gain[...]).astype(bf16)
    drive = dot(normed, w_state[...]).astype(bf16)
    ordered = dot(row_order(False).astype(bf16), drive).astype(bf16)
    drive_out[...] = ordered
    inject = dot(ordered, in_high[...]) + dot(ordered, in_low[...])
    run_re, run_im = inject[:SUBS, :STATE_WIDTH], inject[:SUBS, STATE_WIDTH:]
    s_re[:SUBS, :] = run_re
    s_im[:SUBS, :] = run_im
    for step in range(1, STEPS):
        rows = slice(step * SUBS, (step + 1) * SUBS)
        tr, ti = a_re[rows, :], a_im[rows, :]
        run_re, run_im = (
            tr * run_re - ti * run_im + inject[rows, :STATE_WIDTH],
            tr * run_im + ti * run_re + inject[rows, STATE_WIDTH:],
        )
        s_re[rows, :] = run_re
        s_im[rows, :] = run_im
    last = slice(ROWS - SUBS, ROWS)
    last_re, last_im = m_re[last, :], m_im[last, :]
    in_re = in_im = jnp.zeros((1, STATE_WIDTH), f32)
    mult_re, mult_im = jnp.ones((1, STATE_WIDTH), f32), jnp.zeros((1, STATE_WIDTH), f32)
    for sub in range(SUBS):
        x_re[sub : sub + 1, :] = in_re
        x_im[sub : sub + 1, :] = in_im
        x_re[SUBS + sub : SUBS + sub + 1, :] = mult_re
        x_im[SUBS + sub : SUBS + sub + 1, :] = mult_im
        tr, ti = last_re[sub : sub + 1], last_im[sub : sub + 1]
        in_re, in_im = (
            tr * in_re - ti * in_im + run_re[sub : sub + 1],
            tr * in_im + ti * in_re + run_im[sub : sub + 1],
        )
        mult_re, mult_im = tr * mult_re - ti * mult_im, tr * mult_im + ti * mult_re
    parts = [
        member[:, tile * LANES : (tile + 1) * LANES]
        for member in (mult_re, mult_im, in_re, in_im)
        for tile in range(STATE_WIDTH // LANES)
    ]
    element = jnp.concatenate(parts, axis=0).astype(bf16)
    keep[3 * ROWS :, :] = element
    send[3 * ROWS :, :] = element

    lane = lax.broadcasted_iota(jnp.int32, (ROWS, LANES), 1)
    first_half = lane % QK_DIM < QK_DIM // 2
    cos, sin = cosine[...], sine[...]

    def turned(half):
        other = jnp.where(
            first_half,
            pltpu.roll(half, LANES - QK_DIM // 2, 1),
            pltpu.roll(half, QK_DIM // 2, 1),
        )
        return half * cos + other * sin

    def put(at, first, second):
        rows = slice(at * ROWS, (at + 1) * ROWS)
        keep[rows, :] = jnp.where(head == 0, first, second)
        send[rows, :] = jnp.where(head == 0, second, first)

    query = dot(normed, w_query[...])
    key = dot(normed, w_key[...])
    value = dot(normed, w_value[...])
    put(0, turned(key[:, :LANES]).astype(bf16), turned(key[:, LANES:]).astype(bf16))
    put(1, value[:, :LANES].astype(bf16), value[:, LANES:].astype(bf16))
    put(
        2,
        turned(query[:, :LANES]).astype(bf16) * QK_DIM**-0.5,
        turned(query[:, LANES:]).astype(bf16) * QK_DIM**-0.5,
    )


def attention_kernel(place, mix, sub_gain, keep, got, *rest):
    passed = rest[: RING - 1]
    out_keep, out_send, scores, peak, total, numerator = rest[RING - 1 :]
    depth, head = place[0], place[1]
    pair = 2 * ROWS
    query = jnp.concatenate([keep[2 * ROWS : 3 * ROWS, :], got[2 * ROWS : 3 * ROWS, :]], axis=0)
    queries = (query[:, :QK_DIM], query[:, QK_DIM:])
    row = lax.broadcasted_iota(jnp.int32, (pair, pair), 0)
    column = lax.broadcasted_iota(jnp.int32, (pair, pair), 1)

    def segment(index):
        block = jnp.where(index < ROWS, head, 1 - head)
        return block * (ROWS // SEGMENT) + index % ROWS // SEGMENT

    allowed = segment(column) <= segment(row)
    own_key = jnp.concatenate([keep[:ROWS, :], got[:ROWS, :]], axis=0)
    own_value = jnp.concatenate([keep[ROWS:pair, :], got[ROWS:pair, :]], axis=0)
    for c in range(2):
        raw = dot_nt(queries[c], own_key[:, c * QK_DIM : (c + 1) * QK_DIM])
        masked = jnp.where(allowed, raw, MASK_FLOOR)
        scores[c, 0] = masked
        peak[c] = jnp.maximum(masked[:, :LANES], masked[:, LANES:])
    for k in range(1, RING):

        @pl.when(k <= depth)
        def _():
            for c in range(2):
                keys = passed[k - 1][:pair, c * QK_DIM : (c + 1) * QK_DIM]
                raw = dot_nt(queries[c], keys)
                scores[c, k] = raw
                peak[c] = jnp.maximum(peak[c], jnp.maximum(raw[:, :LANES], raw[:, LANES:]))

    tops = [jnp.max(peak[c], axis=-1, keepdims=True) for c in range(2)]
    for c in range(2):
        weight = jnp.exp(scores[c, 0] - tops[c])
        total[c] = weight[:, :LANES] + weight[:, LANES:]
        numerator[c] = dot(weight.astype(bf16), own_value)
    for k in range(1, RING):

        @pl.when(k <= depth)
        def _():
            for c in range(2):
                weight = jnp.exp(scores[c, k] - tops[c])
                total[c] += weight[:, :LANES] + weight[:, LANES:]
                numerator[c] += dot(weight.astype(bf16), passed[k - 1][pair : 2 * pair, :])

    mapped = [numerator[c] / jnp.sum(total[c], axis=-1, keepdims=True) for c in range(2)]
    difference = mapped[0] - mix[head] * mapped[1]
    mean = jnp.mean(difference * difference, axis=-1, keepdims=True)
    out = difference * lax.rsqrt(mean + EPSILON) * sub_gain[...] * (1.0 - LAMBDA_INIT)
    out_keep[...] = out[:ROWS].astype(bf16)
    out_send[...] = out[ROWS:].astype(bf16)


def state_kernel(place, start, got, *rest):
    passed = rest[: RING - 1]
    s_re, s_im, m_re, m_im, x_re, x_im, drive, skip, out_high, out_low, out, states = rest[RING - 1 :]
    depth, head = place[0], place[1]
    run_re, run_im = start[0:1, :], start[1:2, :]

    def member(ref, base, index):
        tiles = STATE_WIDTH // LANES
        rows = [ref[base + index * tiles + t : base + index * tiles + t + 1, :] for t in range(tiles)]
        return jnp.concatenate(rows, axis=1).astype(f32)

    def advance(carry, ref, base, use):
        re, im = carry
        mr, mi, ar, ai = [member(ref, base, i) for i in range(4)]
        new_re, new_im = mr * re - mi * im + ar, mr * im + mi * re + ai
        return jnp.where(use, new_re, re), jnp.where(use, new_im, im)

    carry = (run_re, run_im)
    pair = 4 * ROWS
    for k in range(RING - 1, 0, -1):
        use = k <= depth
        ref = passed[k - 1]
        mine = [member(ref, pair, i) for i in range(4)]
        other = [member(ref, pair + EL_ROWS, i) for i in range(4)]
        early = [jnp.where(head == 0, a, b) for a, b in zip(mine, other)]
        late = [jnp.where(head == 0, b, a) for a, b in zip(mine, other)]
        for mr, mi, ar, ai in (early, late):
            re, im = carry
            new_re, new_im = mr * re - mi * im + ar, mr * im + mi * re + ai
            carry = jnp.where(use, new_re, re), jnp.where(use, new_im, im)
    carry = advance(carry, got, 3 * ROWS, head == 1)
    in_re, in_im = carry
    pr, pi = x_re[SUBS:, :], x_im[SUBS:, :]
    add_re = x_re[:SUBS, :] + pr * in_re - pi * in_im
    add_im = x_im[:SUBS, :] + pr * in_im + pi * in_re
    for step in range(STEPS):
        rows = slice(step * SUBS, (step + 1) * SUBS)
        mr, mi = m_re[rows, :], m_im[rows, :]
        states[rows, :STATE_WIDTH] = s_re[rows, :] + mr * add_re - mi * add_im
        states[rows, STATE_WIDTH:] = s_im[rows, :] + mr * add_im + mi * add_re
    high, low = split_two(states[...])
    mixed = (
        dot(high, out_high[...])
        + dot(low, out_high[...])
        + dot(high, out_low[...])
        + skip[...] * drive[...].astype(f32)
    )
    result = jax.nn.gelu(mixed).astype(bf16)
    out[...] = dot(row_order(True).astype(bf16), result).astype(bf16)


def output_kernel(place, state, kept, came, weights, out):
    first = place[1] == 0
    mine, other = kept[...], came[...]
    acts = jnp.concatenate(
        [state[...], jnp.where(first, mine, other), jnp.where(first, other, mine)], axis=1
    )
    out[...] = dot_nt(acts, weights[...]).astype(bf16)


VMEM = pl.BlockSpec(memory_space=pltpu.VMEM)
SMEM = pl.BlockSpec(memory_space=pltpu.SMEM)


def call(body, name, out_shapes, smem, args, scratch=()):
    specs = [SMEM if i in smem else VMEM for i in range(len(args))]
    return pl.pallas_call(
        body,
        name=name,
        out_shape=[jax.ShapeDtypeStruct(s, d) for s, d in out_shapes],
        in_specs=specs,
        out_specs=[VMEM] * len(out_shapes),
        scratch_shapes=list(scratch),
        compiler_params=pltpu.CompilerParams(vmem_limit_bytes=48 * 1024 * 1024),
    )(*args)


def sent_to_all(x, axis):
    copies = jnp.broadcast_to(x, (lax.axis_size(axis), *x.shape))
    return lax.all_to_all(copies, axis, split_axis=0, concat_axis=0, tiled=True)


def swapped(x, axis):
    return lax.ppermute(x, axis, [(0, 1), (1, 0)])


def block_diagonal(maps):
    eye = jnp.eye(GROUPS, dtype=f32)
    return jnp.einsum("cgab,gk->gackb", maps, eye, precision=lax.Precision.HIGHEST)


def local(
    tokens,
    norm_gain,
    w_query,
    w_key,
    w_value,
    w_state_in,
    decay_rate,
    rotation,
    extra_decay,
    in_map,
    out_map,
    skip_gain,
    init_state,
    mix_lambda,
    sub_gain,
    w_out_state,
    w_out_attn,
):
    depth, head, core = lax.axis_index("z"), lax.axis_index("h"), lax.axis_index("c")
    sequence = lax.axis_index("q") * 2 + core
    place = jnp.stack([depth, head]).astype(jnp.int32)
    gathered = sent_to_all(tokens, "tp").reshape(ROWS, tokens.shape[1])

    positions = ((depth * 2 + head) * ROWS + jnp.arange(ROWS, dtype=jnp.int32)).astype(f32)
    lane = jnp.arange(LANES, dtype=jnp.int32)
    inverse = ROTARY_BASE ** (-2.0 * (lane % (QK_DIM // 2)).astype(f32) / QK_DIM)
    angles = positions[:, None] * inverse[None, :]
    cosine_table = jnp.cos(angles)
    sine_table = jnp.where(lane % QK_DIM < QK_DIM // 2, -1.0, 1.0)[None, :] * jnp.sin(angles)

    in_scale = jnp.sqrt(-jnp.expm1(-2.0 * decay_rate))
    scaled_in = jnp.swapaxes(in_map * in_scale[None, :, :, None], 2, 3)
    in_high, in_low = split_two(block_diagonal(scaled_in).reshape(GROUPS * GROUP, 2 * STATE_WIDTH))
    signed_out = jnp.swapaxes(out_map, 2, 3) * jnp.array([1.0, -1.0], f32)[:, None, None, None]
    out_high, out_low = split_two(
        jnp.einsum(
            "cgnp,gk->cgnkp",
            signed_out,
            jnp.eye(GROUPS, dtype=f32),
            precision=lax.Precision.HIGHEST,
        ).reshape(2 * STATE_WIDTH, GROUPS * GROUP)
    )
    flat = (1, STATE_WIDTH)
    wide = ((ROWS, STATE_WIDTH), f32)
    trans = call(
        transitions_kernel,
        "transitions",
        [wide] * 4,
        (),
        (
            extra_decay,
            decay_rate.reshape(flat),
            jnp.cos(rotation).reshape(flat),
            jnp.sin(rotation).reshape(flat),
        ),
    )
    weights = jnp.concatenate((w_out_state, w_out_attn), axis=0).T
    start = lax.dynamic_index_in_dim(init_state, sequence, 0, keepdims=False).reshape(
        2, STATE_WIDTH
    )

    payload = ((3 * ROWS + EL_ROWS, LANES), bf16)
    keep, send, s_re, s_im, x_re, x_im, drive = call(
        project_kernel,
        "project",
        [payload, payload, wide, wide]
        + [((2 * SUBS, STATE_WIDTH), f32)] * 2
        + [((ROWS, GROUPS * GROUP), bf16)],
        (0,),
        (
            place,
            gathered,
            norm_gain.reshape(1, -1),
            w_query,
            w_key,
            w_value,
            w_state_in,
            cosine_table,
            sine_table,
            in_high,
            in_low,
            *trans,
        ),
    )
    got = swapped(send, "h")
    weights, gathered = lax.optimization_barrier((weights, gathered))
    weight_blocks = sent_to_all(weights, ("z", "h", "q"))

    shared = jnp.concatenate(
        (
            keep[:ROWS],
            got[:ROWS],
            keep[ROWS : 2 * ROWS],
            got[ROWS : 2 * ROWS],
            keep[3 * ROWS :],
            got[3 * ROWS :],
        ),
        axis=0,
    )
    by_distance = {
        k: lax.ppermute(shared, "z", [(i, i + k) for i in range(RING - k)])
        for k in range(RING - 1, 0, -1)
    }
    passed = [by_distance[k] for k in range(1, RING)]

    pair = (2, 2 * ROWS, LANES)
    out_keep, out_send = call(
        attention_kernel,
        "attention",
        [((ROWS, LANES), bf16)] * 2,
        (0, 1),
        (place, mix_lambda, sub_gain.reshape(1, -1), keep, got, *passed),
        [pltpu.VMEM((2, RING, 2 * ROWS, 2 * ROWS), f32)] + [pltpu.VMEM(pair, f32)] * 3,
    )
    came = swapped(out_send, "h")

    (state_out,) = call(
        state_kernel,
        "state",
        [((ROWS, GROUPS * GROUP), bf16)],
        (0,),
        (
            place,
            start,
            got,
            *passed,
            s_re,
            s_im,
            trans[2],
            trans[3],
            x_re,
            x_im,
            drive,
            skip_gain.reshape(1, -1),
            out_high,
            out_low,
        ),
        [pltpu.VMEM((ROWS, 2 * STATE_WIDTH), f32)],
    )

    other_blocks = swapped(weight_blocks, "c")
    per_block = weights.shape[0]
    mine = weight_blocks.reshape(-1, per_block, weights.shape[1])
    other = other_blocks.reshape(-1, per_block, weights.shape[1])
    full = jnp.where(
        core == 0, jnp.stack((mine, other), axis=1), jnp.stack((other, mine), axis=1)
    ).reshape(-1, weights.shape[1])

    (partial,) = call(
        output_kernel,
        "output",
        [((ROWS, full.shape[0]), bf16)],
        (0,),
        (place, state_out, out_keep, came, full),
    )
    blocks = partial.reshape(lax.axis_size("tp"), tokens.shape[0], -1)
    shares = lax.all_to_all(blocks, "tp", 0, 0, tiled=True)
    return jnp.sum(shares.astype(f32), axis=0).astype(bf16)


def solution(mesh):
    split = Mesh(
        mesh.devices.reshape(8, 2, 4, 2, mesh.shape["tp"]), ("z", "h", "q", "c", "tp")
    )
    return jax.shard_map(
        local,
        mesh=split,
        in_specs=(
            P(SP_TP, None),
            P(),
            P(None, "tp"),
            P(None, "tp"),
            P(None, "tp"),
            P(None, "tp"),
            P("tp", None),
            P("tp", None),
            P(SP, "tp"),
            P(None, "tp", None, None),
            P(None, "tp", None, None),
            P("tp", None),
            P(None, None, "tp", None),
            P("tp"),
            P(),
            P("tp", SP),
            P("tp", SP),
        ),
        out_specs=P(SP_TP, None),
        check_vma=False,
    )
```

```python
import jax
import jax.numpy as jnp
from jax import lax
from jax.experimental import pallas as pl
from jax.experimental.pallas import tpu as pltpu
from jax.sharding import Mesh
from jax.sharding import PartitionSpec as P

SP = ("z", "h", "q", "c")
SP_TP = ("z", "h", "q", "c", "tp")

EPSILON = 1e-06
ROTARY_BASE = 10000.0
LAMBDA_INIT = 0.2
MASK_FLOOR = -1e30
ROWS = 128
SUBS = 8
STEPS = ROWS // SUBS
LANES = 128
QK_DIM = 64
SEGMENT = 64
STATE_WIDTH = 512
GROUPS = 8
GROUP = 16
STATES = 64
EL_ROWS = 16
RING = 8


f32 = jnp.float32
bf16 = jnp.bfloat16


def dot(a, b):
    return jnp.dot(a, b, preferred_element_type=f32)


def dot_nt(a, b):
    return lax.dot_general(a, b, (((1,), (1,)), ((), ())), preferred_element_type=f32)


def split_two(x):
    high = x.astype(bf16)
    return high, (x - high.astype(f32)).astype(bf16)


def row_order(transposed):
    first = lax.broadcasted_iota(jnp.int32, (ROWS, ROWS), 0)
    second = lax.broadcasted_iota(jnp.int32, (ROWS, ROWS), 1)
    row, token = (second, first) if transposed else (first, second)
    return (row % SUBS) * STEPS + row // SUBS == token


def flat_rows(x):
    twice = jnp.concatenate([x, x], axis=1)
    low = lax.broadcasted_iota(jnp.int32, (1, LANES), 1) < STATES
    tiles = [
        jnp.where(low, twice[2 * t : 2 * t + 1], twice[2 * t + 1 : 2 * t + 2])
        for t in range(GROUPS // 2)
    ]
    return jnp.concatenate(tiles, axis=1)


def prelude_kernel(
    extra,
    decay,
    cosine,
    sine,
    in_scale,
    in_map,
    out_map,
    trans,
    product,
    last,
    in_split,
    out_split,
):
    group = lax.broadcasted_iota(jnp.int32, (GROUPS, STATE_WIDTH), 0)
    lane = lax.broadcasted_iota(jnp.int32, (GROUPS, STATE_WIDTH), 1)
    widen = (lane // STATES == group).astype(f32)
    highest = lax.Precision.HIGHEST
    ordered = jnp.dot(
        row_order(False).astype(f32), extra[...], precision=highest, preferred_element_type=f32
    )
    wide = jnp.dot(ordered, widen, precision=highest, preferred_element_type=f32)
    magnitude = jnp.exp(wide - flat_rows(decay[...]))
    real, imag = magnitude * flat_rows(cosine[...]), magnitude * flat_rows(sine[...])
    trans[:, :STATE_WIDTH] = real
    trans[:, STATE_WIDTH:] = imag
    run_re, run_im = real[:SUBS], imag[:SUBS]
    product[:SUBS, :STATE_WIDTH] = run_re
    product[:SUBS, STATE_WIDTH:] = run_im
    for step in range(1, STEPS):
        rows = slice(step * SUBS, (step + 1) * SUBS)
        tr, ti = real[rows], imag[rows]
        run_re, run_im = tr * run_re - ti * run_im, tr * run_im + ti * run_re
        product[rows, :STATE_WIDTH] = run_re
        product[rows, STATE_WIDTH:] = run_im
    last[:, :STATE_WIDTH] = run_re
    last[:, STATE_WIDTH:] = run_im

    row = lax.broadcasted_iota(jnp.int32, (GROUPS * GROUP, STATE_WIDTH), 0)
    column = lax.broadcasted_iota(jnp.int32, (GROUPS * GROUP, STATE_WIDTH), 1)
    own_group = row // GROUP == column // STATES
    scale = flat_rows(in_scale[...])

    def spread(compact):
        twice = jnp.concatenate([compact, compact], axis=1)
        return jnp.concatenate([twice] * (STATE_WIDTH // LANES), axis=1)

    for part in range(2):
        columns = slice(part * STATE_WIDTH, (part + 1) * STATE_WIDTH)
        high, low = split_two(jnp.where(own_group, spread(in_map[part]) * scale, 0.0))
        in_split[0, :, columns] = high
        in_split[1, :, columns] = low
        sign = 1.0 if part == 0 else -1.0
        high, low = split_two(jnp.where(own_group, spread(out_map[part]) * sign, 0.0))
        out_split[0, :, columns] = high
        out_split[1, :, columns] = low


def scan_blocks(inject, trans, last, store):
    run_re, run_im = inject[:SUBS, :STATE_WIDTH], inject[:SUBS, STATE_WIDTH:]
    store(slice(0, SUBS), run_re, run_im)
    for step in range(1, STEPS):
        rows = slice(step * SUBS, (step + 1) * SUBS)
        tr, ti = trans[rows, :STATE_WIDTH], trans[rows, STATE_WIDTH:]
        run_re, run_im = (
            tr * run_re - ti * run_im + inject[rows, :STATE_WIDTH],
            tr * run_im + ti * run_re + inject[rows, STATE_WIDTH:],
        )
        store(rows, run_re, run_im)
    last_re, last_im = last[:, :STATE_WIDTH], last[:, STATE_WIDTH:]
    add = (jnp.zeros((1, STATE_WIDTH), f32), jnp.zeros((1, STATE_WIDTH), f32))
    mult = (jnp.ones((1, STATE_WIDTH), f32), jnp.zeros((1, STATE_WIDTH), f32))
    starts = []
    for sub in range(SUBS):
        starts.append((*mult, *add))
        one = slice(sub, sub + 1)
        tr, ti = last_re[one], last_im[one]
        add = (
            tr * add[0] - ti * add[1] + run_re[one],
            tr * add[1] + ti * add[0] + run_im[one],
        )
        mult = (tr * mult[0] - ti * mult[1], tr * mult[1] + ti * mult[0])
    return starts, (*mult, *add)


def inject_of(drive, in_split):
    return dot(drive, in_split[0]) + dot(drive, in_split[1])


def project_kernel(
    place,
    tokens,
    gain,
    w_query,
    w_key,
    last,
    cosine,
    sine,
    w_value_far,
    w_state_far,
    trans_far,
    split_far,
    keep,
    send,
    drive_out,
    w_value,
    w_state,
    trans,
    in_split,
    arrived,
):
    copies = [
        pltpu.make_async_copy(far, near, arrived.at[i])
        for i, (far, near) in enumerate(
            (
                (w_state_far, w_state),
                (split_far, in_split),
                (trans_far, trans),
                (w_value_far, w_value),
            )
        )
    ]
    for copy in copies:
        copy.start()
    head = place[1]
    wide = tokens[...].astype(f32)
    scale = lax.rsqrt(jnp.mean(wide * wide, axis=-1, keepdims=True) + EPSILON)
    normed = (wide * scale * gain[...]).astype(bf16)
    copies[0].wait()
    drive = dot(normed, w_state[...]).astype(bf16)
    ordered = dot(row_order(False).astype(bf16), drive).astype(bf16)
    drive_out[...] = ordered
    copies[1].wait()
    copies[2].wait()
    copies[3].wait()
    inject = inject_of(ordered, in_split)
    _, element_parts = scan_blocks(inject, trans, last, lambda rows, re, im: None)
    parts = [
        member[:, tile * LANES : (tile + 1) * LANES]
        for member in element_parts
        for tile in range(STATE_WIDTH // LANES)
    ]
    element = jnp.concatenate(parts, axis=0).astype(bf16)
    keep[3 * ROWS :, :] = element
    send[3 * ROWS :, :] = element

    lane = lax.broadcasted_iota(jnp.int32, (ROWS, LANES), 1)
    first_half = lane % QK_DIM < QK_DIM // 2
    cos, sin = cosine[...], sine[...]

    def turned(half):
        other = jnp.where(
            first_half,
            pltpu.roll(half, LANES - QK_DIM // 2, 1),
            pltpu.roll(half, QK_DIM // 2, 1),
        )
        return half * cos + other * sin

    def put(at, first, second):
        rows = slice(at * ROWS, (at + 1) * ROWS)
        keep[rows, :] = jnp.where(head == 0, first, second)
        send[rows, :] = jnp.where(head == 0, second, first)

    query = dot(normed, w_query[...])
    key = dot(normed, w_key[...])
    value = dot(normed, w_value[...])
    put(0, turned(key[:, :LANES]).astype(bf16), turned(key[:, LANES:]).astype(bf16))
    put(1, value[:, :LANES].astype(bf16), value[:, LANES:].astype(bf16))
    put(
        2,
        turned(query[:, :LANES]).astype(bf16) * QK_DIM**-0.5,
        turned(query[:, LANES:]).astype(bf16) * QK_DIM**-0.5,
    )


def join_kernel(keep, got, out):
    for part in range(2):
        rows = slice(part * ROWS, (part + 1) * ROWS)
        out[2 * part * ROWS : (2 * part + 1) * ROWS, :] = keep[rows, :]
        out[(2 * part + 1) * ROWS : 2 * (part + 1) * ROWS, :] = got[rows, :]
    out[4 * ROWS : 4 * ROWS + EL_ROWS, :] = keep[3 * ROWS :, :]
    out[4 * ROWS + EL_ROWS :, :] = got[3 * ROWS :, :]


def attention_kernel(place, mix, sub_gain, keep, got, *rest):
    passed = rest[: RING - 1]
    out_keep, out_send, scores, peak, total, numerator = rest[RING - 1 :]
    depth, head = place[0], place[1]
    pair = 2 * ROWS
    query = jnp.concatenate([keep[2 * ROWS : 3 * ROWS, :], got[2 * ROWS : 3 * ROWS, :]], axis=0)
    queries = (query[:, :QK_DIM], query[:, QK_DIM:])
    row = lax.broadcasted_iota(jnp.int32, (pair, pair), 0)
    column = lax.broadcasted_iota(jnp.int32, (pair, pair), 1)

    def segment(index):
        block = jnp.where(index < ROWS, head, 1 - head)
        return block * (ROWS // SEGMENT) + index % ROWS // SEGMENT

    allowed = segment(column) <= segment(row)
    own_key = jnp.concatenate([keep[:ROWS, :], got[:ROWS, :]], axis=0)
    own_value = jnp.concatenate([keep[ROWS:pair, :], got[ROWS:pair, :]], axis=0)
    for c in range(2):
        raw = dot_nt(queries[c], own_key[:, c * QK_DIM : (c + 1) * QK_DIM])
        masked = jnp.where(allowed, raw, MASK_FLOOR)
        scores[c, 0] = masked
        peak[c] = jnp.maximum(masked[:, :LANES], masked[:, LANES:])
    for k in range(1, RING):

        @pl.when(k <= depth)
        def _():
            for c in range(2):
                keys = passed[k - 1][:pair, c * QK_DIM : (c + 1) * QK_DIM]
                raw = dot_nt(queries[c], keys)
                scores[c, k] = raw
                peak[c] = jnp.maximum(peak[c], jnp.maximum(raw[:, :LANES], raw[:, LANES:]))

    tops = [jnp.max(peak[c], axis=-1, keepdims=True) for c in range(2)]
    for c in range(2):
        weight = jnp.exp(scores[c, 0] - tops[c])
        total[c] = weight[:, :LANES] + weight[:, LANES:]
        numerator[c] = dot(weight.astype(bf16), own_value)
    for k in range(1, RING):

        @pl.when(k <= depth)
        def _():
            for c in range(2):
                weight = jnp.exp(scores[c, k] - tops[c])
                total[c] += weight[:, :LANES] + weight[:, LANES:]
                numerator[c] += dot(weight.astype(bf16), passed[k - 1][pair : 2 * pair, :])

    mapped = [numerator[c] / jnp.sum(total[c], axis=-1, keepdims=True) for c in range(2)]
    difference = mapped[0] - mix[head] * mapped[1]
    mean = jnp.mean(difference * difference, axis=-1, keepdims=True)
    out = difference * lax.rsqrt(mean + EPSILON) * sub_gain[...] * (1.0 - LAMBDA_INIT)
    out_keep[...] = out[:ROWS].astype(bf16)
    out_send[...] = out[ROWS:].astype(bf16)


def state_kernel(place, start, got, *rest):
    passed = rest[: RING - 1]
    (
        last,
        drive,
        skip,
        trans_far,
        product_far,
        in_far,
        out_far,
        out,
        trans,
        product,
        in_split,
        out_split,
        states,
        arrived,
    ) = rest[RING - 1 :]
    copies = [
        pltpu.make_async_copy(far, near, arrived.at[i])
        for i, (far, near) in enumerate(
            (
                (in_far, in_split),
                (trans_far, trans),
                (product_far, product),
                (out_far, out_split),
            )
        )
    ]
    for copy in copies:
        copy.start()
    depth, head = place[0], place[1]
    run_re, run_im = start[0:1, :], start[1:2, :]

    def member(ref, base, index):
        tiles = STATE_WIDTH // LANES
        rows = [ref[base + index * tiles + t : base + index * tiles + t + 1, :] for t in range(tiles)]
        return jnp.concatenate(rows, axis=1).astype(f32)

    def advance(carry, ref, base, use):
        re, im = carry
        mr, mi, ar, ai = [member(ref, base, i) for i in range(4)]
        new_re, new_im = mr * re - mi * im + ar, mr * im + mi * re + ai
        return jnp.where(use, new_re, re), jnp.where(use, new_im, im)

    carry = (run_re, run_im)
    pair = 4 * ROWS
    for k in range(RING - 1, 0, -1):
        use = k <= depth
        ref = passed[k - 1]
        mine = [member(ref, pair, i) for i in range(4)]
        other = [member(ref, pair + EL_ROWS, i) for i in range(4)]
        early = [jnp.where(head == 0, a, b) for a, b in zip(mine, other)]
        late = [jnp.where(head == 0, b, a) for a, b in zip(mine, other)]
        for mr, mi, ar, ai in (early, late):
            re, im = carry
            new_re, new_im = mr * re - mi * im + ar, mr * im + mi * re + ai
            carry = jnp.where(use, new_re, re), jnp.where(use, new_im, im)
    carry = advance(carry, got, 3 * ROWS, head == 1)
    in_re, in_im = carry
    for copy in copies:
        copy.wait()

    def store(rows, re, im):
        states[rows, :STATE_WIDTH] = re
        states[rows, STATE_WIDTH:] = im

    starts, _ = scan_blocks(inject_of(drive[...], in_split), trans, last, store)
    add_re = jnp.concatenate([ar + mr * in_re - mi * in_im for mr, mi, ar, ai in starts], axis=0)
    add_im = jnp.concatenate([ai + mr * in_im + mi * in_re for mr, mi, ar, ai in starts], axis=0)
    for step in range(STEPS):
        rows = slice(step * SUBS, (step + 1) * SUBS)
        mr, mi = product[rows, :STATE_WIDTH], product[rows, STATE_WIDTH:]
        states[rows, :STATE_WIDTH] += mr * add_re - mi * add_im
        states[rows, STATE_WIDTH:] += mr * add_im + mi * add_re
    high, low = split_two(states[...])
    mixed = (
        dot_nt(high, out_split[0])
        + dot_nt(low, out_split[0])
        + dot_nt(high, out_split[1])
        + skip[...] * drive[...].astype(f32)
    )
    result = jax.nn.gelu(mixed).astype(bf16)
    out[...] = dot(row_order(True).astype(bf16), result).astype(bf16)


def output_kernel(place, state, kept, came, own, swapped_in, out, full):
    first = place[1] == 0
    mine, other = kept[...], came[...]
    acts = jnp.concatenate(
        [state[...], jnp.where(first, mine, other), jnp.where(first, other, mine)], axis=1
    )
    low_core = place[2] == 0
    for block in range(own.shape[0]):
        here, there = own[block], swapped_in[block]
        at = block % RING * 8 + block // RING
        full[at, 0] = jnp.where(low_core, here, there)
        full[at, 1] = jnp.where(low_core, there, here)
    weights = full[...].reshape(2 * own.shape[0] * own.shape[1], own.shape[2])
    out[...] = dot_nt(acts, weights).astype(bf16)


VMEM = pl.BlockSpec(memory_space=pltpu.VMEM)
SMEM = pl.BlockSpec(memory_space=pltpu.SMEM)
FAR = pl.BlockSpec(memory_space=pltpu.HBM)


def call(body, name, out_shapes, smem, args, scratch=(), far=0):
    near = len(args) - far
    specs = [SMEM if i in smem else VMEM if i < near else FAR for i in range(len(args))]
    return pl.pallas_call(
        body,
        name=name,
        out_shape=[jax.ShapeDtypeStruct(s, d) for s, d in out_shapes],
        in_specs=specs,
        out_specs=[VMEM] * len(out_shapes),
        scratch_shapes=list(scratch),
        compiler_params=pltpu.CompilerParams(vmem_limit_bytes=20 * 1024 * 1024),
    )(*args)


def sent_to_all(x, axis):
    copies = jnp.broadcast_to(x, (lax.axis_size(axis), *x.shape))
    return lax.all_to_all(copies, axis, split_axis=0, concat_axis=0, tiled=True)


def swapped(x, axis):
    return lax.ppermute(x, axis, [(0, 1), (1, 0)])


def local(
    tokens,
    norm_gain,
    w_query,
    w_key,
    w_value,
    w_state_in,
    decay_rate,
    rotation,
    extra_decay,
    in_map,
    out_map,
    skip_gain,
    init_state,
    mix_lambda,
    sub_gain,
    w_out_state,
    w_out_attn,
):
    depth, head, core = lax.axis_index("z"), lax.axis_index("h"), lax.axis_index("c")
    sequence = lax.axis_index("q") * 2 + core
    place = jnp.stack([depth, head, core]).astype(jnp.int32)
    with jax.named_scope("tok_send"):
        gathered = sent_to_all(tokens, "tp").reshape(ROWS, tokens.shape[1])

    with jax.named_scope("prelude"):
        positions = ((depth * 2 + head) * ROWS + jnp.arange(ROWS, dtype=jnp.int32)).astype(f32)
        lane = jnp.arange(LANES, dtype=jnp.int32)
        inverse = ROTARY_BASE ** (-2.0 * (lane % (QK_DIM // 2)).astype(f32) / QK_DIM)
        angles = positions[:, None] * inverse[None, :]
        cosine_table = jnp.cos(angles)
        sine_table = jnp.where(lane % QK_DIM < QK_DIM // 2, -1.0, 1.0)[None, :] * jnp.sin(angles)
        maps = (2, GROUPS * GROUP, STATES)
        wide = ((ROWS, 2 * STATE_WIDTH), f32)
        diagonal = ((2, GROUPS * GROUP, 2 * STATE_WIDTH), bf16)
        trans, product, last, in_split, out_split = call(
            prelude_kernel,
            "prelude",
            [wide, wide, ((SUBS, 2 * STATE_WIDTH), f32), diagonal, diagonal],
            (),
            (
                extra_decay,
                decay_rate,
                jnp.cos(rotation),
                jnp.sin(rotation),
                jnp.sqrt(-jnp.expm1(-2.0 * decay_rate)),
                jnp.swapaxes(in_map, 2, 3).reshape(maps),
                out_map.reshape(maps),
            ),
        )
        weights = jnp.concatenate((w_out_state, w_out_attn), axis=0).T
        start = lax.dynamic_index_in_dim(init_state, sequence, 0, keepdims=False).reshape(
            2, STATE_WIDTH
        )

    payload = ((3 * ROWS + EL_ROWS, LANES), bf16)
    with jax.named_scope("project"):
        keep, send, drive = call(
            project_kernel,
            "project",
            [payload, payload, ((ROWS, GROUPS * GROUP), bf16)],
            (0,),
            (
                place,
                gathered,
                norm_gain.reshape(1, -1),
                w_query,
                w_key,
                last,
                cosine_table,
                sine_table,
                w_value,
                w_state_in,
                trans,
                in_split,
            ),
            [
                pltpu.VMEM(w_value.shape, bf16),
                pltpu.VMEM(w_state_in.shape, bf16),
                pltpu.VMEM(wide[0], f32),
                pltpu.VMEM(diagonal[0], bf16),
                pltpu.SemaphoreType.DMA((4,)),
            ],
            far=4,
        )
    with jax.named_scope("swap_h"):
        got = swapped(send, "h")
    weights, keep = lax.optimization_barrier((weights, keep))
    with jax.named_scope("weights_z"):
        weight_rows = sent_to_all(weights, "z").reshape(-1, weights.shape[1])

    with jax.named_scope("join"):
        (shared,) = call(
            join_kernel, "join", [((4 * ROWS + 2 * EL_ROWS, LANES), bf16)], (), (keep, got)
        )

    def along(name, x, pairs):
        with jax.named_scope(name):
            return lax.ppermute(x, "z", pairs)

    up = lambda by, first=0: [(i, i + by) for i in range(first, RING - by)]
    two = along("z_two", shared, up(2))
    six = along("z_six", shared, [(0, 6), (1, 7), (2, 0)])
    one = along("z_one", shared, up(1))
    seven = along("z_seven", shared, [(0, 7)])
    four = along("z_four", two, up(2, 2))
    three = along("z_three", two, up(1, 2))
    five = along("z_five", six, [(6, 5), (7, 6), (0, 7)])
    passed = [one, two, three, four, five, six, seven]
    weight_rows, _ = lax.optimization_barrier((weight_rows, two))
    with jax.named_scope("weights_y"):
        weight_blocks = sent_to_all(weight_rows, ("h", "q"))

    pair = (2, 2 * ROWS, LANES)
    with jax.named_scope("attention"):
        out_keep, out_send = call(
            attention_kernel,
            "attention",
            [((ROWS, LANES), bf16)] * 2,
            (0, 1),
            (place, mix_lambda, sub_gain.reshape(1, -1), keep, got, *passed),
            [pltpu.VMEM((2, RING, 2 * ROWS, 2 * ROWS), f32)] + [pltpu.VMEM(pair, f32)] * 3,
        )
    with jax.named_scope("swap_back"):
        came = swapped(out_send, "h")

    with jax.named_scope("state"):
        (state_out,) = call(
            state_kernel,
            "state",
            [((ROWS, GROUPS * GROUP), bf16)],
            (0,),
            (
                place,
                start,
                got,
                *passed,
                last,
                drive,
                skip_gain.reshape(1, -1),
                trans,
                product,
                in_split,
                out_split,
            ),
            [
                pltpu.VMEM(wide[0], f32),
                pltpu.VMEM(wide[0], f32),
                pltpu.VMEM(diagonal[0], bf16),
                pltpu.VMEM(diagonal[0], bf16),
                pltpu.VMEM(wide[0], f32),
                pltpu.SemaphoreType.DMA((4,)),
            ],
            far=4,
        )

    weight_blocks, out_keep = lax.optimization_barrier((weight_blocks, out_keep))
    with jax.named_scope("weights_c"):
        other_blocks = swapped(weight_blocks, "c")
    width = w_out_attn.shape[1]
    blocks = (-1, width, weights.shape[1])

    with jax.named_scope("output"):
        (partial,) = call(
            output_kernel,
            "output",
            [((ROWS, RING * 2 * 8 * width), bf16)],
            (0,),
            (
                place,
                state_out,
                out_keep,
                came,
                weight_blocks.reshape(blocks),
                other_blocks.reshape(blocks),
            ),
            [pltpu.VMEM((RING * 8, 2, width, weights.shape[1]), bf16)],
        )
    with jax.named_scope("reduce_tp"):
        parts = partial.reshape(lax.axis_size("tp"), tokens.shape[0], -1)
        shares = lax.all_to_all(parts, "tp", 0, 0, tiled=True)
        return jnp.sum(shares.astype(f32), axis=0).astype(bf16)


def solution(mesh):
    split = Mesh(
        mesh.devices.reshape(8, 2, 4, 2, mesh.shape["tp"]), ("z", "h", "q", "c", "tp")
    )
    return jax.shard_map(
        local,
        mesh=split,
        in_specs=(
            P(SP_TP, None),
            P(),
            P(None, "tp"),
            P(None, "tp"),
            P(None, "tp"),
            P(None, "tp"),
            P("tp", None),
            P("tp", None),
            P(SP, "tp"),
            P(None, "tp", None, None),
            P(None, "tp", None, None),
            P("tp", None),
            P(None, None, "tp", None),
            P("tp"),
            P(),
            P("tp", SP),
            P("tp", SP),
        ),
        out_specs=P(SP_TP, None),
        check_vma=False,
    )
```

```python
import jax
import jax.numpy as jnp
from jax import lax
from jax.experimental import pallas as pl
from jax.experimental.pallas import tpu as pltpu
from jax.sharding import Mesh
from jax.sharding import PartitionSpec as P

SP = ("z", "h", "q", "c")
SP_TP = ("z", "h", "q", "c", "tp")

EPSILON = 1e-06
ROTARY_BASE = 10000.0
LAMBDA_INIT = 0.2
MASK_FLOOR = -1e30
ROWS = 128
SUBS = 8
STEPS = ROWS // SUBS
LANES = 128
QK_DIM = 64
SEGMENT = 64
STATE_WIDTH = 512
GROUPS = 8
GROUP = 16
STATES = 64
EL_ROWS = 16
RING = 8


f32 = jnp.float32
bf16 = jnp.bfloat16


def dot(a, b):
    return jnp.dot(a, b, preferred_element_type=f32)


def dot_nt(a, b):
    return lax.dot_general(a, b, (((1,), (1,)), ((), ())), preferred_element_type=f32)


def split_two(x):
    high = x.astype(bf16)
    return high, (x - high.astype(f32)).astype(bf16)


def row_order(transposed):
    first = lax.broadcasted_iota(jnp.int32, (ROWS, ROWS), 0)
    second = lax.broadcasted_iota(jnp.int32, (ROWS, ROWS), 1)
    row, token = (second, first) if transposed else (first, second)
    return (row % SUBS) * STEPS + row // SUBS == token


def flat_rows(x):
    twice = jnp.concatenate([x, x], axis=1)
    low = lax.broadcasted_iota(jnp.int32, (1, LANES), 1) < STATES
    tiles = [
        jnp.where(low, twice[2 * t : 2 * t + 1], twice[2 * t + 1 : 2 * t + 2])
        for t in range(GROUPS // 2)
    ]
    return jnp.concatenate(tiles, axis=1)


def wide_transitions(extra, decay, cosine, sine):
    group = lax.broadcasted_iota(jnp.int32, (GROUPS, STATE_WIDTH), 0)
    lane = lax.broadcasted_iota(jnp.int32, (GROUPS, STATE_WIDTH), 1)
    widen = (lane // STATES == group).astype(f32)
    highest = lax.Precision.HIGHEST
    ordered = jnp.dot(
        row_order(False).astype(f32), extra, precision=highest, preferred_element_type=f32
    )
    wide = jnp.dot(ordered, widen, precision=highest, preferred_element_type=f32)
    magnitude = jnp.exp(wide - flat_rows(decay))
    return magnitude * flat_rows(cosine), magnitude * flat_rows(sine)


def running_products(real, imag, store):
    run_re, run_im = real[:SUBS], imag[:SUBS]
    store(slice(0, SUBS), run_re, run_im)
    for step in range(1, STEPS):
        rows = slice(step * SUBS, (step + 1) * SUBS)
        tr, ti = real[rows], imag[rows]
        run_re, run_im = tr * run_re - ti * run_im, tr * run_im + ti * run_re
        store(rows, run_re, run_im)
    return run_re, run_im


def block_diagonal(compact, scale):
    row = lax.broadcasted_iota(jnp.int32, (GROUPS * GROUP, STATE_WIDTH), 0)
    column = lax.broadcasted_iota(jnp.int32, (GROUPS * GROUP, STATE_WIDTH), 1)
    twice = jnp.concatenate([compact, compact], axis=1)
    spread = jnp.concatenate([twice] * (STATE_WIDTH // LANES), axis=1)
    return split_two(jnp.where(row // GROUP == column // STATES, spread * scale, 0.0))


def put_pair(ref, rows, re, im):
    ref[rows, :STATE_WIDTH] = re
    ref[rows, STATE_WIDTH:] = im


def put_split(ref, maps, scales):
    for part in range(2):
        columns = slice(part * STATE_WIDTH, (part + 1) * STATE_WIDTH)
        high, low = block_diagonal(maps[part], scales[part])
        ref[0, :, columns] = high
        ref[1, :, columns] = low


ALL = slice(None)


def prelude_kernel(extra, decay, cosine, sine, in_scale, in_map, trans, last, in_split):
    real, imag = wide_transitions(extra[...], decay[...], cosine[...], sine[...])
    put_pair(trans, ALL, real, imag)
    put_pair(last, ALL, *running_products(real, imag, lambda rows, re, im: None))
    scale = flat_rows(in_scale[...])
    put_split(in_split, in_map, (scale, scale))


def fan_kernel(one, out):
    for i in range(out.shape[0]):
        out[i] = one[...]


def scan_blocks(inject, trans, last, store):
    run_re, run_im = inject[:SUBS, :STATE_WIDTH], inject[:SUBS, STATE_WIDTH:]
    store(slice(0, SUBS), run_re, run_im)
    for step in range(1, STEPS):
        rows = slice(step * SUBS, (step + 1) * SUBS)
        tr, ti = trans[rows, :STATE_WIDTH], trans[rows, STATE_WIDTH:]
        run_re, run_im = (
            tr * run_re - ti * run_im + inject[rows, :STATE_WIDTH],
            tr * run_im + ti * run_re + inject[rows, STATE_WIDTH:],
        )
        store(rows, run_re, run_im)
    last_re, last_im = last
    add = (jnp.zeros((1, STATE_WIDTH), f32), jnp.zeros((1, STATE_WIDTH), f32))
    mult = (jnp.ones((1, STATE_WIDTH), f32), jnp.zeros((1, STATE_WIDTH), f32))
    starts = []
    for sub in range(SUBS):
        starts.append((*mult, *add))
        one = slice(sub, sub + 1)
        tr, ti = last_re[one], last_im[one]
        add = (
            tr * add[0] - ti * add[1] + run_re[one],
            tr * add[1] + ti * add[0] + run_im[one],
        )
        mult = (tr * mult[0] - ti * mult[1], tr * mult[1] + ti * mult[0])
    return starts, (*mult, *add)


def inject_of(drive, in_split):
    return dot(drive, in_split[0]) + dot(drive, in_split[1])


def project_kernel(
    place,
    tokens,
    gain,
    w_query,
    w_key,
    last,
    cosine,
    sine,
    trans,
    in_split,
    w_value_far,
    w_state_far,
    keep,
    send,
    drive_out,
    w_value,
    w_state,
    arrived,
):
    copies = [
        pltpu.make_async_copy(far, near, arrived.at[i])
        for i, (far, near) in enumerate(
            (
                (w_state_far, w_state),
                (w_value_far, w_value),
            )
        )
    ]
    for copy in copies:
        copy.start()
    head = place[1]
    wide = tokens[...].astype(f32)
    scale = lax.rsqrt(jnp.mean(wide * wide, axis=-1, keepdims=True) + EPSILON)
    normed = (wide * scale * gain[...]).astype(bf16)
    copies[0].wait()
    drive = dot(normed, w_state[...]).astype(bf16)
    ordered = dot(row_order(False).astype(bf16), drive).astype(bf16)
    drive_out[...] = ordered
    inject = inject_of(ordered, in_split)
    _, element_parts = scan_blocks(
        inject,
        trans,
        (last[:, :STATE_WIDTH], last[:, STATE_WIDTH:]),
        lambda rows, re, im: None,
    )
    parts = [
        member[:, tile * LANES : (tile + 1) * LANES]
        for member in element_parts
        for tile in range(STATE_WIDTH // LANES)
    ]
    element = jnp.concatenate(parts, axis=0).astype(bf16)
    keep[3 * ROWS :, :] = element
    send[3 * ROWS :, :] = element

    lane = lax.broadcasted_iota(jnp.int32, (ROWS, LANES), 1)
    first_half = lane % QK_DIM < QK_DIM // 2
    cos, sin = cosine[...], sine[...]

    def turned(half):
        other = jnp.where(
            first_half,
            pltpu.roll(half, LANES - QK_DIM // 2, 1),
            pltpu.roll(half, QK_DIM // 2, 1),
        )
        return half * cos + other * sin

    def put(at, first, second):
        rows = slice(at * ROWS, (at + 1) * ROWS)
        keep[rows, :] = jnp.where(head == 0, first, second)
        send[rows, :] = jnp.where(head == 0, second, first)

    query = dot(normed, w_query[...])
    key = dot(normed, w_key[...])
    copies[1].wait()
    value = dot(normed, w_value[...])
    put(0, turned(key[:, :LANES]).astype(bf16), turned(key[:, LANES:]).astype(bf16))
    put(1, value[:, :LANES].astype(bf16), value[:, LANES:].astype(bf16))
    put(
        2,
        turned(query[:, :LANES]).astype(bf16) * QK_DIM**-0.5,
        turned(query[:, LANES:]).astype(bf16) * QK_DIM**-0.5,
    )


def join_kernel(keep, got, out):
    for part in range(2):
        rows = slice(part * ROWS, (part + 1) * ROWS)
        out[2 * part * ROWS : (2 * part + 1) * ROWS, :] = keep[rows, :]
        out[(2 * part + 1) * ROWS : 2 * (part + 1) * ROWS, :] = got[rows, :]
    out[4 * ROWS : 4 * ROWS + EL_ROWS, :] = keep[3 * ROWS :, :]
    out[4 * ROWS + EL_ROWS :, :] = got[3 * ROWS :, :]


def attention_kernel(place, mix, sub_gain, keep, got, *rest):
    passed = rest[: RING - 1]
    out_keep, out_send, elements, scores, peak, total, numerator = rest[RING - 1 :]
    depth, head = place[0], place[1]
    pair = 2 * ROWS
    for k in range(RING - 1):
        elements[2 * EL_ROWS * k : 2 * EL_ROWS * (k + 1), :] = passed[k][2 * pair :, :]
    query = jnp.concatenate([keep[2 * ROWS : 3 * ROWS, :], got[2 * ROWS : 3 * ROWS, :]], axis=0)
    queries = (query[:, :QK_DIM], query[:, QK_DIM:])
    row = lax.broadcasted_iota(jnp.int32, (pair, pair), 0)
    column = lax.broadcasted_iota(jnp.int32, (pair, pair), 1)

    def segment(index):
        block = jnp.where(index < ROWS, head, 1 - head)
        return block * (ROWS // SEGMENT) + index % ROWS // SEGMENT

    allowed = segment(column) <= segment(row)
    own_key = jnp.concatenate([keep[:ROWS, :], got[:ROWS, :]], axis=0)
    own_value = jnp.concatenate([keep[ROWS:pair, :], got[ROWS:pair, :]], axis=0)
    for c in range(2):
        raw = dot_nt(queries[c], own_key[:, c * QK_DIM : (c + 1) * QK_DIM])
        masked = jnp.where(allowed, raw, MASK_FLOOR)
        scores[c, 0] = masked
        peak[c] = jnp.maximum(masked[:, :LANES], masked[:, LANES:])
    for k in range(1, RING):

        @pl.when(k <= depth)
        def _():
            for c in range(2):
                keys = passed[k - 1][:pair, c * QK_DIM : (c + 1) * QK_DIM]
                raw = dot_nt(queries[c], keys)
                scores[c, k] = raw
                peak[c] = jnp.maximum(peak[c], jnp.maximum(raw[:, :LANES], raw[:, LANES:]))

    tops = [jnp.max(peak[c], axis=-1, keepdims=True) for c in range(2)]
    for c in range(2):
        weight = jnp.exp(scores[c, 0] - tops[c])
        total[c] = weight[:, :LANES] + weight[:, LANES:]
        numerator[c] = dot(weight.astype(bf16), own_value)
    for k in range(1, RING):

        @pl.when(k <= depth)
        def _():
            for c in range(2):
                weight = jnp.exp(scores[c, k] - tops[c])
                total[c] += weight[:, :LANES] + weight[:, LANES:]
                numerator[c] += dot(weight.astype(bf16), passed[k - 1][pair : 2 * pair, :])

    mapped = [numerator[c] / jnp.sum(total[c], axis=-1, keepdims=True) for c in range(2)]
    difference = mapped[0] - mix[head] * mapped[1]
    mean = jnp.mean(difference * difference, axis=-1, keepdims=True)
    out = difference * lax.rsqrt(mean + EPSILON) * sub_gain[...] * (1.0 - LAMBDA_INIT)
    out_keep[...] = out[:ROWS].astype(bf16)
    out_send[...] = out[ROWS:].astype(bf16)


def state_kernel(
    place,
    init,
    got,
    elements,
    drive,
    skip,
    extra,
    decay,
    cosine,
    sine,
    in_scale,
    in_map,
    out_map,
    out,
    trans,
    product,
    in_split,
    out_split,
    states,
):
    depth, head, sequence = place[0], place[1], place[3]
    real, imag = wide_transitions(extra[...], decay[...], cosine[...], sine[...])
    put_pair(trans, ALL, real, imag)
    last = running_products(real, imag, lambda rows, re, im: put_pair(product, rows, re, im))
    scale = flat_rows(in_scale[...])
    put_split(in_split, in_map, (scale, scale))
    put_split(out_split, out_map, (1.0, -1.0))
    run_re, run_im = flat_rows(init[sequence, 0]), flat_rows(init[sequence, 1])

    def member(ref, base, index):
        tiles = STATE_WIDTH // LANES
        rows = [ref[base + index * tiles + t : base + index * tiles + t + 1, :] for t in range(tiles)]
        return jnp.concatenate(rows, axis=1).astype(f32)

    def advance(carry, ref, base, use):
        re, im = carry
        mr, mi, ar, ai = [member(ref, base, i) for i in range(4)]
        new_re, new_im = mr * re - mi * im + ar, mr * im + mi * re + ai
        return jnp.where(use, new_re, re), jnp.where(use, new_im, im)

    carry = (run_re, run_im)
    for k in range(RING - 1, 0, -1):
        use = k <= depth
        base = 2 * EL_ROWS * (k - 1)
        mine = [member(elements, base, i) for i in range(4)]
        other = [member(elements, base + EL_ROWS, i) for i in range(4)]
        early = [jnp.where(head == 0, a, b) for a, b in zip(mine, other)]
        late = [jnp.where(head == 0, b, a) for a, b in zip(mine, other)]
        for mr, mi, ar, ai in (early, late):
            re, im = carry
            new_re, new_im = mr * re - mi * im + ar, mr * im + mi * re + ai
            carry = jnp.where(use, new_re, re), jnp.where(use, new_im, im)
    carry = advance(carry, got, 3 * ROWS, head == 1)
    in_re, in_im = carry
    starts, _ = scan_blocks(
        inject_of(drive[...], in_split),
        trans,
        last,
        lambda rows, re, im: put_pair(states, rows, re, im),
    )
    add_re = jnp.concatenate([ar + mr * in_re - mi * in_im for mr, mi, ar, ai in starts], axis=0)
    add_im = jnp.concatenate([ai + mr * in_im + mi * in_re for mr, mi, ar, ai in starts], axis=0)
    for step in range(STEPS):
        rows = slice(step * SUBS, (step + 1) * SUBS)
        mr, mi = product[rows, :STATE_WIDTH], product[rows, STATE_WIDTH:]
        states[rows, :STATE_WIDTH] += mr * add_re - mi * add_im
        states[rows, STATE_WIDTH:] += mr * add_im + mi * add_re
    high, low = split_two(states[...])
    lane = lax.broadcasted_iota(jnp.int32, (GROUP, LANES), 1)
    spread = (lane % GROUP == lax.broadcasted_iota(jnp.int32, (GROUP, LANES), 0)).astype(f32)
    tiled = jnp.dot(
        skip[...], spread, precision=lax.Precision.HIGHEST, preferred_element_type=f32
    )
    own = lax.broadcasted_iota(jnp.int32, (GROUPS, LANES), 1) // GROUP
    own = own == lax.broadcasted_iota(jnp.int32, (GROUPS, LANES), 0)
    skip_row = jnp.sum(jnp.where(own, tiled, 0.0), axis=0, keepdims=True)
    mixed = (
        dot_nt(high, out_split[0])
        + dot_nt(low, out_split[0])
        + dot_nt(high, out_split[1])
        + skip_row * drive[...].astype(f32)
    )
    result = jax.nn.gelu(mixed).astype(bf16)
    out[...] = dot(row_order(True).astype(bf16), result).astype(bf16)


def output_kernel(place, state, kept, came, own, swapped_in, out, full):
    first = place[1] == 0
    mine, other = kept[...], came[...]
    acts = jnp.concatenate(
        [state[...], jnp.where(first, mine, other), jnp.where(first, other, mine)], axis=1
    )
    low_core = place[2] == 0
    for block in range(own.shape[0]):
        here, there = own[block], swapped_in[block]
        at = block % RING * 8 + block // RING
        full[at, 0] = jnp.where(low_core, here, there)
        full[at, 1] = jnp.where(low_core, there, here)
    weights = full[...].reshape(2 * own.shape[0] * own.shape[1], own.shape[2])
    out[...] = dot_nt(acts, weights).astype(bf16)


VMEM = pl.BlockSpec(memory_space=pltpu.VMEM)
SMEM = pl.BlockSpec(memory_space=pltpu.SMEM)
FAR = pl.BlockSpec(memory_space=pltpu.HBM)


def call(body, out_shapes, smem, args, scratch=(), far=0):
    near = len(args) - far
    specs = [SMEM if i in smem else VMEM if i < near else FAR for i in range(len(args))]
    return pl.pallas_call(
        body,
        out_shape=[jax.ShapeDtypeStruct(s, d) for s, d in out_shapes],
        in_specs=specs,
        out_specs=[VMEM] * len(out_shapes),
        scratch_shapes=list(scratch),
        compiler_params=pltpu.CompilerParams(vmem_limit_bytes=20 * 1024 * 1024),
    )(*args)


def sent_to_all(x, axis):
    (copies,) = call(fan_kernel, [((lax.axis_size(axis), *x.shape), x.dtype)], (), (x,))
    return lax.all_to_all(copies, axis, split_axis=0, concat_axis=0, tiled=True)


def in_hbm(x):
    return pltpu.with_memory_space_constraint(x, pltpu.HBM)


def swapped(x, axis):
    return lax.ppermute(x, axis, [(0, 1), (1, 0)])


def local(
    tokens,
    norm_gain,
    w_query,
    w_key,
    w_value,
    w_state_in,
    decay_rate,
    rotation,
    extra_decay,
    in_map,
    out_map,
    skip_gain,
    init_state,
    mix_lambda,
    sub_gain,
    w_out_state,
    w_out_attn,
):
    depth, head, core = lax.axis_index("z"), lax.axis_index("h"), lax.axis_index("c")
    sequence = lax.axis_index("q") * 2 + core
    place = jnp.stack([depth, head, core, sequence]).astype(jnp.int32)
    gathered = sent_to_all(tokens, "tp").reshape(ROWS, tokens.shape[1])

    positions = ((depth * 2 + head) * ROWS + jnp.arange(ROWS, dtype=jnp.int32)).astype(f32)
    lane = jnp.arange(LANES, dtype=jnp.int32)
    inverse = ROTARY_BASE ** (-2.0 * (lane % (QK_DIM // 2)).astype(f32) / QK_DIM)
    angles = positions[:, None] * inverse[None, :]
    cosine_table = jnp.cos(angles)
    sine_table = jnp.where(lane % QK_DIM < QK_DIM // 2, -1.0, 1.0)[None, :] * jnp.sin(angles)
    maps = (2, GROUPS * GROUP, STATES)
    wide = ((ROWS, 2 * STATE_WIDTH), f32)
    diagonal = ((2, GROUPS * GROUP, 2 * STATE_WIDTH), bf16)
    state_params = (
        extra_decay,
        decay_rate,
        jnp.cos(rotation),
        jnp.sin(rotation),
        jnp.sqrt(-jnp.expm1(-2.0 * decay_rate)),
        jnp.swapaxes(in_map, 2, 3).reshape(maps),
    )
    trans, last, in_split = call(
        prelude_kernel, [wide, ((SUBS, 2 * STATE_WIDTH), f32), diagonal], (), state_params
    )
    weights = jnp.concatenate((w_out_state, w_out_attn), axis=0).T

    payload = ((3 * ROWS + EL_ROWS, LANES), bf16)
    keep, send, drive = call(
        project_kernel,
        [payload, payload, ((ROWS, GROUPS * GROUP), bf16)],
        (0,),
        (
            place,
            gathered,
            norm_gain.reshape(1, -1),
            w_query,
            w_key,
            last,
            cosine_table,
            sine_table,
            trans,
            in_split,
            in_hbm(w_value),
            in_hbm(w_state_in),
        ),
        [
            pltpu.VMEM(w_value.shape, bf16),
            pltpu.VMEM(w_state_in.shape, bf16),
            pltpu.SemaphoreType.DMA((2,)),
        ],
        far=2,
    )
    got = swapped(send, "h")
    weights, keep = lax.optimization_barrier((weights, keep))
    weight_rows = sent_to_all(weights, "z").reshape(-1, weights.shape[1])

    (shared,) = call(join_kernel, [((4 * ROWS + 2 * EL_ROWS, LANES), bf16)], (), (keep, got))

    def along(x, pairs):
        return lax.ppermute(x, "z", pairs)

    up = lambda by, first=0: [(i, i + by) for i in range(first, RING - by)]
    two = along(shared, up(2))
    six = along(shared, [(0, 6), (1, 7), (2, 0)])
    one = along(shared, up(1))
    seven = along(shared, [(0, 7)])
    four = along(two, up(2, 2))
    three = along(two, up(1, 2))
    five = along(six, [(6, 5), (7, 6), (0, 7)])
    passed = [one, two, three, four, five, six, seven]
    weight_blocks = sent_to_all(weight_rows, ("h", "q"))

    pair = (2, 2 * ROWS, LANES)
    out_keep, out_send, elements = call(
        attention_kernel,
        [((ROWS, LANES), bf16)] * 2 + [((2 * EL_ROWS * (RING - 1), LANES), bf16)],
        (0, 1),
        (place, mix_lambda, sub_gain.reshape(1, -1), keep, got, *passed),
        [pltpu.VMEM((2, RING, 2 * ROWS, 2 * ROWS), f32)] + [pltpu.VMEM(pair, f32)] * 3,
    )
    came = swapped(out_send, "h")

    (state_out,) = call(
        state_kernel,
        [((ROWS, GROUPS * GROUP), bf16)],
        (0,),
        (place, init_state, got, elements, drive, skip_gain, *state_params, out_map.reshape(maps)),
        [
            pltpu.VMEM(wide[0], f32),
            pltpu.VMEM(wide[0], f32),
            pltpu.VMEM(diagonal[0], bf16),
            pltpu.VMEM(diagonal[0], bf16),
            pltpu.VMEM(wide[0], f32),
        ],
    )

    weight_blocks, out_keep = lax.optimization_barrier((weight_blocks, out_keep))
    other_blocks = swapped(weight_blocks, "c")
    width = w_out_attn.shape[1]
    blocks = (-1, width, weights.shape[1])

    (partial,) = call(
        output_kernel,
        [((ROWS, RING * 2 * 8 * width), bf16)],
        (0,),
        (
            place,
            state_out,
            out_keep,
            came,
            weight_blocks.reshape(blocks),
            other_blocks.reshape(blocks),
        ),
        [pltpu.VMEM((RING * 8, 2, width, weights.shape[1]), bf16)],
    )
    parts = partial.reshape(lax.axis_size("tp"), tokens.shape[0], -1)
    shares = lax.all_to_all(parts, "tp", 0, 0, tiled=True)
    return jnp.sum(shares.astype(f32), axis=0).astype(bf16)


def solution(mesh):
    split = Mesh(
        mesh.devices.reshape(8, 2, 4, 2, mesh.shape["tp"]), ("z", "h", "q", "c", "tp")
    )

    return jax.shard_map(
        local,
        mesh=split,
        in_specs=(
            P(SP_TP, None),
            P(),
            P(None, "tp"),
            P(None, "tp"),
            P(None, "tp"),
            P(None, "tp"),
            P("tp", None),
            P("tp", None),
            P(SP, "tp"),
            P(None, "tp", None, None),
            P(None, "tp", None, None),
            P("tp", None),
            P(None, None, "tp", None),
            P("tp"),
            P(),
            P("tp", SP),
            P("tp", SP),
        ),
        out_specs=P(SP_TP, None),
        check_vma=False,
    )
```

```python
import jax
import jax.numpy as jnp
from jax import lax
from jax.experimental import pallas as pl
from jax.experimental.pallas import tpu as pltpu
from jax.sharding import Mesh
from jax.sharding import PartitionSpec as P

SP = ("z", "h", "q", "c")
Y = ("h", "q")
SP_TP = ("z", "h", "q", "c", "tp")

EPSILON = 1e-06
ROTARY_BASE = 10000.0
LAMBDA_INIT = 0.2
MASK_FLOOR = -1e30
ROWS = 128
SUBS = 8
STEPS = ROWS // SUBS
LANES = 128
QK_DIM = 64
SEGMENT = 64
STATE_WIDTH = 512
GROUPS = 8
GROUP = 16
STATES = 64
EL_ROWS = 16
RING = 8


f32 = jnp.float32
bf16 = jnp.bfloat16


def dot(a, b):
    return jnp.dot(a, b, preferred_element_type=f32)


def dot_nt(a, b):
    return lax.dot_general(a, b, (((1,), (1,)), ((), ())), preferred_element_type=f32)


def split_two(x):
    high = x.astype(bf16)
    return high, (x - high.astype(f32)).astype(bf16)


def row_order(transposed):
    first = lax.broadcasted_iota(jnp.int32, (ROWS, ROWS), 0)
    second = lax.broadcasted_iota(jnp.int32, (ROWS, ROWS), 1)
    row, token = (second, first) if transposed else (first, second)
    return (row % SUBS) * STEPS + row // SUBS == token


def flat_rows(x):
    twice = jnp.concatenate([x, x], axis=1)
    low = lax.broadcasted_iota(jnp.int32, (1, LANES), 1) < STATES
    tiles = [
        jnp.where(low, twice[2 * t : 2 * t + 1], twice[2 * t + 1 : 2 * t + 2])
        for t in range(GROUPS // 2)
    ]
    return jnp.concatenate(tiles, axis=1)


def wide_transitions(extra, decay, cosine, sine):
    group = lax.broadcasted_iota(jnp.int32, (GROUPS, STATE_WIDTH), 0)
    lane = lax.broadcasted_iota(jnp.int32, (GROUPS, STATE_WIDTH), 1)
    widen = (lane // STATES == group).astype(f32)
    highest = lax.Precision.HIGHEST
    ordered = jnp.dot(
        row_order(False).astype(f32), extra, precision=highest, preferred_element_type=f32
    )
    wide = jnp.dot(ordered, widen, precision=highest, preferred_element_type=f32)
    magnitude = jnp.exp(wide - flat_rows(decay))
    return magnitude * flat_rows(cosine), magnitude * flat_rows(sine)


def running_products(real, imag, store):
    run_re, run_im = real[:SUBS], imag[:SUBS]
    store(slice(0, SUBS), run_re, run_im)
    for step in range(1, STEPS):
        rows = slice(step * SUBS, (step + 1) * SUBS)
        tr, ti = real[rows], imag[rows]
        run_re, run_im = tr * run_re - ti * run_im, tr * run_im + ti * run_re
        store(rows, run_re, run_im)
    return run_re, run_im


def block_diagonal(compact, scale):
    row = lax.broadcasted_iota(jnp.int32, (GROUPS * GROUP, STATE_WIDTH), 0)
    column = lax.broadcasted_iota(jnp.int32, (GROUPS * GROUP, STATE_WIDTH), 1)
    twice = jnp.concatenate([compact, compact], axis=1)
    spread = jnp.concatenate([twice] * (STATE_WIDTH // LANES), axis=1)
    return split_two(jnp.where(row // GROUP == column // STATES, spread * scale, 0.0))


def put_pair(ref, rows, re, im):
    ref[rows, :STATE_WIDTH] = re
    ref[rows, STATE_WIDTH:] = im


def put_split(ref, maps, scales):
    for part in range(2):
        columns = slice(part * STATE_WIDTH, (part + 1) * STATE_WIDTH)
        high, low = block_diagonal(maps[part], scales[part])
        ref[0, :, columns] = high
        ref[1, :, columns] = low


ALL = slice(None)


def prelude_kernel(extra, decay, cosine, sine, in_scale, in_map, trans, in_split):
    real, imag = wide_transitions(extra[...], decay[...], cosine[...], sine[...])
    put_pair(trans, slice(0, ROWS), real, imag)
    ends = running_products(real, imag, lambda rows, re, im: None)
    put_pair(trans, slice(ROWS, ROWS + SUBS), *ends)
    scale = flat_rows(in_scale[...])
    put_split(in_split, in_map, (scale, scale))


def fan_kernel(one, out):
    for i in range(out.shape[0]):
        out[i] = one[...]


def scan_blocks(inject, trans, last, store):
    run_re, run_im = inject[:SUBS, :STATE_WIDTH], inject[:SUBS, STATE_WIDTH:]
    store(slice(0, SUBS), run_re, run_im)
    for step in range(1, STEPS):
        rows = slice(step * SUBS, (step + 1) * SUBS)
        tr, ti = trans[rows, :STATE_WIDTH], trans[rows, STATE_WIDTH:]
        run_re, run_im = (
            tr * run_re - ti * run_im + inject[rows, :STATE_WIDTH],
            tr * run_im + ti * run_re + inject[rows, STATE_WIDTH:],
        )
        store(rows, run_re, run_im)
    last_re, last_im = last
    add = (jnp.zeros((1, STATE_WIDTH), f32), jnp.zeros((1, STATE_WIDTH), f32))
    mult = (jnp.ones((1, STATE_WIDTH), f32), jnp.zeros((1, STATE_WIDTH), f32))
    starts = []
    for sub in range(SUBS):
        starts.append((*mult, *add))
        one = slice(sub, sub + 1)
        tr, ti = last_re[one], last_im[one]
        add = (
            tr * add[0] - ti * add[1] + run_re[one],
            tr * add[1] + ti * add[0] + run_im[one],
        )
        mult = (tr * mult[0] - ti * mult[1], tr * mult[1] + ti * mult[0])
    return starts, (*mult, *add)


def inject_of(drive, in_split):
    return dot(drive, in_split[0]) + dot(drive, in_split[1])


def project_kernel(
    place,
    tokens,
    gain,
    w_query,
    w_key_far,
    tables_far,
    w_state_far,
    split_far,
    trans_far,
    w_value_far,
    keep,
    send,
    drive_far,
    w_key,
    tables,
    w_state,
    in_split,
    trans,
    w_value,
    drive_near,
    arrived,
):
    far = (w_key_far, tables_far, w_state_far, split_far, trans_far, w_value_far)
    near = (w_key, tables, w_state, in_split, trans, w_value)
    copies = [
        pltpu.make_async_copy(source, target, arrived.at[i])
        for i, (source, target) in enumerate(zip(far, near))
    ]
    for copy in copies:
        copy.start()
    head = place[1]
    wide = tokens[...].astype(f32)
    scale = lax.rsqrt(jnp.mean(wide * wide, axis=-1, keepdims=True) + EPSILON)
    normed = (wide * scale * gain[...]).astype(bf16)

    def put(at, first, second):
        place_rows = slice(at * ROWS, (at + 1) * ROWS)
        keep[place_rows, :] = jnp.where(head == 0, first, second)
        send[place_rows, :] = jnp.where(head == 0, second, first)

    query = dot(normed, w_query[...])
    copies[0].wait()
    key = dot(normed, w_key[...])
    for copy in copies[1:5]:
        copy.wait()
    lane = lax.broadcasted_iota(jnp.int32, (ROWS, LANES), 1)
    first_half = lane % QK_DIM < QK_DIM // 2
    cos, sin = tables[0], tables[1]

    def turned(half):
        other = jnp.where(
            first_half,
            pltpu.roll(half, LANES - QK_DIM // 2, 1),
            pltpu.roll(half, QK_DIM // 2, 1),
        )
        return (half * cos + other * sin).astype(bf16)

    drive = dot(normed, w_state[...]).astype(bf16)
    ordered = dot(row_order(False).astype(bf16), drive).astype(bf16)
    drive_near[...] = ordered
    put(0, turned(key[:, :LANES]), turned(key[:, LANES:]))
    put(
        2,
        turned(query[:, :LANES]) * QK_DIM**-0.5,
        turned(query[:, LANES:]) * QK_DIM**-0.5,
    )
    inject = inject_of(ordered, in_split)
    copies[5].wait()
    leaving = pltpu.make_async_copy(drive_near, drive_far, arrived.at[6])
    leaving.start()
    value = dot(normed, w_value[...])
    put(1, value[:, :LANES].astype(bf16), value[:, LANES:].astype(bf16))
    _, element_parts = scan_blocks(
        inject,
        trans,
        (trans[ROWS:, :STATE_WIDTH], trans[ROWS:, STATE_WIDTH:]),
        lambda where, re, im: None,
    )
    pieces = [
        member[:, tile * LANES : (tile + 1) * LANES]
        for member in element_parts
        for tile in range(STATE_WIDTH // LANES)
    ]
    element = jnp.concatenate(pieces, axis=0).astype(bf16)
    keep[3 * ROWS :, :] = element
    send[3 * ROWS :, :] = element
    leaving.wait()


def join_kernel(keep, got, out):
    for part in range(2):
        rows = slice(part * ROWS, (part + 1) * ROWS)
        out[2 * part * ROWS : (2 * part + 1) * ROWS, :] = keep[rows, :]
        out[(2 * part + 1) * ROWS : 2 * (part + 1) * ROWS, :] = got[rows, :]
    out[4 * ROWS : 4 * ROWS + EL_ROWS, :] = keep[3 * ROWS :, :]
    out[4 * ROWS + EL_ROWS :, :] = got[3 * ROWS :, :]


def attention_kernel(place, mix, sub_gain, keep, got, *rest):
    passed = rest[: RING - 1]
    out_keep, out_send, elements, scores, peak, total, numerator = rest[RING - 1 :]
    depth, head = place[0], place[1]
    pair = 2 * ROWS
    for k in range(RING - 1):
        elements[2 * EL_ROWS * k : 2 * EL_ROWS * (k + 1), :] = passed[k][2 * pair :, :]
    query = jnp.concatenate([keep[2 * ROWS : 3 * ROWS, :], got[2 * ROWS : 3 * ROWS, :]], axis=0)
    queries = (query[:, :QK_DIM], query[:, QK_DIM:])
    row = lax.broadcasted_iota(jnp.int32, (pair, pair), 0)
    column = lax.broadcasted_iota(jnp.int32, (pair, pair), 1)

    def segment(index):
        block = jnp.where(index < ROWS, head, 1 - head)
        return block * (ROWS // SEGMENT) + index % ROWS // SEGMENT

    allowed = segment(column) <= segment(row)
    own_key = jnp.concatenate([keep[:ROWS, :], got[:ROWS, :]], axis=0)
    own_value = jnp.concatenate([keep[ROWS:pair, :], got[ROWS:pair, :]], axis=0)
    for c in range(2):
        raw = dot_nt(queries[c], own_key[:, c * QK_DIM : (c + 1) * QK_DIM])
        masked = jnp.where(allowed, raw, MASK_FLOOR)
        scores[c, 0] = masked
        peak[c] = jnp.maximum(masked[:, :LANES], masked[:, LANES:])
    for k in range(1, RING):

        @pl.when(k <= depth)
        def _():
            for c in range(2):
                keys = passed[k - 1][:pair, c * QK_DIM : (c + 1) * QK_DIM]
                raw = dot_nt(queries[c], keys)
                scores[c, k] = raw
                peak[c] = jnp.maximum(peak[c], jnp.maximum(raw[:, :LANES], raw[:, LANES:]))

    tops = [jnp.max(peak[c], axis=-1, keepdims=True) for c in range(2)]
    for c in range(2):
        weight = jnp.exp(scores[c, 0] - tops[c])
        total[c] = weight[:, :LANES] + weight[:, LANES:]
        numerator[c] = dot(weight.astype(bf16), own_value)
    for k in range(1, RING):

        @pl.when(k <= depth)
        def _():
            for c in range(2):
                weight = jnp.exp(scores[c, k] - tops[c])
                total[c] += weight[:, :LANES] + weight[:, LANES:]
                numerator[c] += dot(weight.astype(bf16), passed[k - 1][pair : 2 * pair, :])

    mapped = [numerator[c] / jnp.sum(total[c], axis=-1, keepdims=True) for c in range(2)]
    difference = mapped[0] - mix[head] * mapped[1]
    mean = jnp.mean(difference * difference, axis=-1, keepdims=True)
    out = difference * lax.rsqrt(mean + EPSILON) * sub_gain[...] * (1.0 - LAMBDA_INIT)
    out_keep[...] = out[:ROWS].astype(bf16)
    out_send[...] = out[ROWS:].astype(bf16)


def state_kernel(
    place,
    init,
    got,
    elements,
    drive,
    skip,
    extra,
    decay,
    cosine,
    sine,
    in_scale,
    in_map,
    out_map,
    out,
    trans,
    product,
    in_split,
    out_split,
    states,
):
    depth, head, sequence = place[0], place[1], place[3]
    real, imag = wide_transitions(extra[...], decay[...], cosine[...], sine[...])
    put_pair(trans, ALL, real, imag)
    last = running_products(real, imag, lambda rows, re, im: put_pair(product, rows, re, im))
    scale = flat_rows(in_scale[...])
    put_split(in_split, in_map, (scale, scale))
    put_split(out_split, out_map, (1.0, -1.0))
    run_re, run_im = flat_rows(init[sequence, 0]), flat_rows(init[sequence, 1])

    def member(ref, base, index):
        tiles = STATE_WIDTH // LANES
        rows = [ref[base + index * tiles + t : base + index * tiles + t + 1, :] for t in range(tiles)]
        return jnp.concatenate(rows, axis=1).astype(f32)

    def advance(carry, ref, base, use):
        re, im = carry
        mr, mi, ar, ai = [member(ref, base, i) for i in range(4)]
        new_re, new_im = mr * re - mi * im + ar, mr * im + mi * re + ai
        return jnp.where(use, new_re, re), jnp.where(use, new_im, im)

    carry = (run_re, run_im)
    for k in range(RING - 1, 0, -1):
        use = k <= depth
        base = 2 * EL_ROWS * (k - 1)
        mine = [member(elements, base, i) for i in range(4)]
        other = [member(elements, base + EL_ROWS, i) for i in range(4)]
        early = [jnp.where(head == 0, a, b) for a, b in zip(mine, other)]
        late = [jnp.where(head == 0, b, a) for a, b in zip(mine, other)]
        for mr, mi, ar, ai in (early, late):
            re, im = carry
            new_re, new_im = mr * re - mi * im + ar, mr * im + mi * re + ai
            carry = jnp.where(use, new_re, re), jnp.where(use, new_im, im)
    carry = advance(carry, got, 3 * ROWS, head == 1)
    in_re, in_im = carry
    starts, _ = scan_blocks(
        inject_of(drive[...], in_split),
        trans,
        last,
        lambda rows, re, im: put_pair(states, rows, re, im),
    )
    add_re = jnp.concatenate([ar + mr * in_re - mi * in_im for mr, mi, ar, ai in starts], axis=0)
    add_im = jnp.concatenate([ai + mr * in_im + mi * in_re for mr, mi, ar, ai in starts], axis=0)
    for step in range(STEPS):
        rows = slice(step * SUBS, (step + 1) * SUBS)
        mr, mi = product[rows, :STATE_WIDTH], product[rows, STATE_WIDTH:]
        states[rows, :STATE_WIDTH] += mr * add_re - mi * add_im
        states[rows, STATE_WIDTH:] += mr * add_im + mi * add_re
    high, low = split_two(states[...])
    lane = lax.broadcasted_iota(jnp.int32, (GROUP, LANES), 1)
    spread = (lane % GROUP == lax.broadcasted_iota(jnp.int32, (GROUP, LANES), 0)).astype(f32)
    tiled = jnp.dot(
        skip[...], spread, precision=lax.Precision.HIGHEST, preferred_element_type=f32
    )
    own = lax.broadcasted_iota(jnp.int32, (GROUPS, LANES), 1) // GROUP
    own = own == lax.broadcasted_iota(jnp.int32, (GROUPS, LANES), 0)
    skip_row = jnp.sum(jnp.where(own, tiled, 0.0), axis=0, keepdims=True)
    mixed = (
        dot_nt(high, out_split[0])
        + dot_nt(low, out_split[0])
        + dot_nt(high, out_split[1])
        + skip_row * drive[...].astype(f32)
    )
    result = jax.nn.gelu(mixed).astype(bf16)
    out[...] = dot(row_order(True).astype(bf16), result).astype(bf16)


def output_kernel(place, state, kept, came, own, swapped_in, out, full):
    first = place[1] == 0
    mine, other = kept[...], came[...]
    acts = jnp.concatenate(
        [state[...], jnp.where(first, mine, other), jnp.where(first, other, mine)], axis=1
    )
    low_core = place[2] == 0
    for block in range(own.shape[0]):
        here, there = own[block], swapped_in[block]
        at = block % RING * 8 + block // RING
        full[at, 0] = jnp.where(low_core, here, there)
        full[at, 1] = jnp.where(low_core, there, here)
    weights = full[...].reshape(2 * own.shape[0] * own.shape[1], own.shape[2])
    out[...] = dot_nt(acts, weights).astype(bf16)


VMEM = pl.BlockSpec(memory_space=pltpu.VMEM)
SMEM = pl.BlockSpec(memory_space=pltpu.SMEM)
FAR = pl.BlockSpec(memory_space=pltpu.HBM)


def call(body, out_shapes, smem, args, scratch=(), far=0, far_out=0):
    near = len(args) - far
    specs = [SMEM if i in smem else VMEM if i < near else FAR for i in range(len(args))]
    return pl.pallas_call(
        body,
        out_shape=[jax.ShapeDtypeStruct(s, d) for s, d in out_shapes],
        in_specs=specs,
        out_specs=[VMEM] * (len(out_shapes) - far_out) + [FAR] * far_out,
        scratch_shapes=list(scratch),
        compiler_params=pltpu.CompilerParams(vmem_limit_bytes=20 * 1024 * 1024),
    )(*args)


def fanned(x, axis):
    shape = (lax.axis_size(axis), *x.shape)
    (copies,) = call(fan_kernel, [(shape, x.dtype)], (), (x,))
    return copies


def in_hbm(x):
    return pltpu.with_memory_space_constraint(x, pltpu.HBM)


def swapped(x, axis):
    return lax.ppermute(x, axis, [(0, 1), (1, 0)])


def local(
    tokens,
    norm_gain,
    w_query,
    w_key,
    w_value,
    w_state_in,
    decay_rate,
    rotation,
    extra_decay,
    in_map,
    out_map,
    skip_gain,
    init_state,
    mix_lambda,
    sub_gain,
    w_out_state,
    w_out_attn,
):
    depth, head, core = lax.axis_index("z"), lax.axis_index("h"), lax.axis_index("c")
    sequence = lax.axis_index("q") * 2 + core
    place = jnp.stack([depth, head, core, sequence]).astype(jnp.int32)
    gathered = lax.all_to_all(fanned(tokens, "tp"), "tp", 0, 0, tiled=True)
    weights = jnp.concatenate((w_out_state, w_out_attn), axis=0).T
    fan_weights = fanned(weights, "z")
    gathered = gathered.reshape(ROWS, tokens.shape[1])

    positions = ((depth * 2 + head) * ROWS + jnp.arange(ROWS, dtype=jnp.int32)).astype(f32)
    lane = jnp.arange(LANES, dtype=jnp.int32)
    inverse = ROTARY_BASE ** (-2.0 * (lane % (QK_DIM // 2)).astype(f32) / QK_DIM)
    angles = positions[:, None] * inverse[None, :]
    cosine_table = jnp.cos(angles)
    sine_table = jnp.where(lane % QK_DIM < QK_DIM // 2, -1.0, 1.0)[None, :] * jnp.sin(angles)
    maps = (2, GROUPS * GROUP, STATES)
    wide = ((ROWS, 2 * STATE_WIDTH), f32)
    diagonal = ((2, GROUPS * GROUP, 2 * STATE_WIDTH), bf16)
    state_params = (
        extra_decay,
        decay_rate,
        jnp.cos(rotation),
        jnp.sin(rotation),
        jnp.sqrt(-jnp.expm1(-2.0 * decay_rate)),
        jnp.swapaxes(in_map, 2, 3).reshape(maps),
    )
    tables = jnp.stack((cosine_table, sine_table))
    trans, in_split = call(
        prelude_kernel, [((ROWS + SUBS, 2 * STATE_WIDTH), f32), diagonal], (), state_params
    )

    fan_weights, gathered, trans, in_split, tables = lax.optimization_barrier(
        (fan_weights, gathered, trans, in_split, tables)
    )
    weight_rows = lax.all_to_all(fan_weights, "z", 0, 0, tiled=True)
    weight_rows = weight_rows.reshape(-1, weights.shape[1])

    payload = ((3 * ROWS + EL_ROWS, LANES), bf16)
    keep, send, drive = call(
        project_kernel,
        [payload, payload, ((ROWS, GROUPS * GROUP), bf16)],
        (0,),
        (
            place,
            gathered,
            norm_gain.reshape(1, -1),
            w_query,
            in_hbm(w_key),
            in_hbm(tables),
            in_hbm(w_state_in),
            in_hbm(in_split),
            in_hbm(trans),
            in_hbm(w_value),
        ),
        [
            pltpu.VMEM(w_key.shape, bf16),
            pltpu.VMEM(tables.shape, f32),
            pltpu.VMEM(w_state_in.shape, bf16),
            pltpu.VMEM(in_split.shape, bf16),
            pltpu.VMEM(trans.shape, f32),
            pltpu.VMEM(w_value.shape, bf16),
            pltpu.VMEM((ROWS, GROUPS * GROUP), bf16),
            pltpu.SemaphoreType.DMA((7,)),
        ],
        far=6,
        far_out=1,
    )
    got = swapped(send, "h")
    (shared,) = call(join_kernel, [((4 * ROWS + 2 * EL_ROWS, LANES), bf16)], (), (keep, got))

    def along(x, pairs):
        return lax.ppermute(x, "z", pairs)

    up = lambda by, first=0: [(i, i + by) for i in range(first, RING - by)]
    two = along(shared, up(2))
    six = along(shared, [(0, 6), (1, 7), (2, 0)])
    one = along(shared, up(1))
    seven = along(shared, [(0, 7)])
    four = along(two, up(2, 2))
    three = along(two, up(1, 2))
    five = along(six, [(6, 5), (7, 6), (0, 7)])
    passed = [one, two, three, four, five, six, seven]
    weight_blocks = lax.all_to_all(fanned(weight_rows, Y), Y, 0, 0, tiled=True)

    pair = (2, 2 * ROWS, LANES)
    out_keep, out_send, elements = call(
        attention_kernel,
        [((ROWS, LANES), bf16)] * 2 + [((2 * EL_ROWS * (RING - 1), LANES), bf16)],
        (0, 1),
        (place, mix_lambda, sub_gain.reshape(1, -1), keep, got, *passed),
        [pltpu.VMEM((2, RING, 2 * ROWS, 2 * ROWS), f32)] + [pltpu.VMEM(pair, f32)] * 3,
    )
    came = swapped(out_send, "h")

    (state_out,) = call(
        state_kernel,
        [((ROWS, GROUPS * GROUP), bf16)],
        (0,),
        (place, init_state, got, elements, drive, skip_gain, *state_params, out_map.reshape(maps)),
        [
            pltpu.VMEM(wide[0], f32),
            pltpu.VMEM(wide[0], f32),
            pltpu.VMEM(diagonal[0], bf16),
            pltpu.VMEM(diagonal[0], bf16),
            pltpu.VMEM(wide[0], f32),
        ],
    )

    other_blocks = swapped(weight_blocks, "c")
    width = w_out_attn.shape[1]
    blocks = (-1, width, weights.shape[1])

    (partial,) = call(
        output_kernel,
        [((ROWS, RING * 2 * 8 * width), bf16)],
        (0,),
        (
            place,
            state_out,
            out_keep,
            came,
            weight_blocks.reshape(blocks),
            other_blocks.reshape(blocks),
        ),
        [pltpu.VMEM((RING * 8, 2, width, weights.shape[1]), bf16)],
    )
    parts = partial.reshape(lax.axis_size("tp"), tokens.shape[0], -1)
    shares = lax.all_to_all(parts, "tp", 0, 0, tiled=True)
    return jnp.sum(shares.astype(f32), axis=0).astype(bf16)


def solution(mesh):
    split = Mesh(
        mesh.devices.reshape(8, 2, 4, 2, mesh.shape["tp"]), ("z", "h", "q", "c", "tp")
    )

    return jax.shard_map(
        local,
        mesh=split,
        in_specs=(
            P(SP_TP, None),
            P(),
            P(None, "tp"),
            P(None, "tp"),
            P(None, "tp"),
            P(None, "tp"),
            P("tp", None),
            P("tp", None),
            P(SP, "tp"),
            P(None, "tp", None, None),
            P(None, "tp", None, None),
            P("tp", None),
            P(None, None, "tp", None),
            P("tp"),
            P(),
            P("tp", SP),
            P("tp", SP),
        ),
        out_specs=P(SP_TP, None),
        check_vma=False,
    )
```

```python
import jax
import jax.numpy as jnp
from jax import lax
from jax.experimental import pallas as pl
from jax.experimental.pallas import tpu as pltpu
from jax.sharding import Mesh
from jax.sharding import PartitionSpec as P

SP = ("z", "h", "q", "c")
Y = ("h", "q")
SP_TP = ("z", "h", "q", "c", "tp")

EPSILON = 1e-06
ROTARY_BASE = 10000.0
LAMBDA_INIT = 0.2
MASK_FLOOR = -1e30
ROWS = 128
SUBS = 8
STEPS = ROWS // SUBS
LANES = 128
QK_DIM = 64
SEGMENT = 64
STATE_WIDTH = 512
GROUPS = 8
GROUP = 16
STATES = 64
EL_ROWS = 16
RING = 8


f32 = jnp.float32
bf16 = jnp.bfloat16


def dot(a, b):
    return jnp.dot(a, b, preferred_element_type=f32)


def dot_nt(a, b):
    return lax.dot_general(a, b, (((1,), (1,)), ((), ())), preferred_element_type=f32)


def split_two(x):
    high = x.astype(bf16)
    return high, (x - high.astype(f32)).astype(bf16)


def row_order(transposed):
    first = lax.broadcasted_iota(jnp.int32, (ROWS, ROWS), 0)
    second = lax.broadcasted_iota(jnp.int32, (ROWS, ROWS), 1)
    row, token = (second, first) if transposed else (first, second)
    return (row % SUBS) * STEPS + row // SUBS == token


def flat_rows(x):
    twice = jnp.concatenate([x, x], axis=1)
    low = lax.broadcasted_iota(jnp.int32, (1, LANES), 1) < STATES
    tiles = [
        jnp.where(low, twice[2 * t : 2 * t + 1], twice[2 * t + 1 : 2 * t + 2])
        for t in range(GROUPS // 2)
    ]
    return jnp.concatenate(tiles, axis=1)


def wide_transitions(extra, decay, cosine, sine):
    group = lax.broadcasted_iota(jnp.int32, (GROUPS, STATE_WIDTH), 0)
    lane = lax.broadcasted_iota(jnp.int32, (GROUPS, STATE_WIDTH), 1)
    widen = (lane // STATES == group).astype(f32)
    highest = lax.Precision.HIGHEST
    ordered = jnp.dot(
        row_order(False).astype(f32), extra, precision=highest, preferred_element_type=f32
    )
    wide = jnp.dot(ordered, widen, precision=highest, preferred_element_type=f32)
    magnitude = jnp.exp(wide - flat_rows(decay))
    return magnitude * flat_rows(cosine), magnitude * flat_rows(sine)


def running_products(real, imag, store):
    run_re, run_im = real[:SUBS], imag[:SUBS]
    store(slice(0, SUBS), run_re, run_im)
    for step in range(1, STEPS):
        rows = slice(step * SUBS, (step + 1) * SUBS)
        tr, ti = real[rows], imag[rows]
        run_re, run_im = tr * run_re - ti * run_im, tr * run_im + ti * run_re
        store(rows, run_re, run_im)
    return run_re, run_im


def block_diagonal(compact, scale):
    row = lax.broadcasted_iota(jnp.int32, (GROUPS * GROUP, STATE_WIDTH), 0)
    column = lax.broadcasted_iota(jnp.int32, (GROUPS * GROUP, STATE_WIDTH), 1)
    twice = jnp.concatenate([compact, compact], axis=1)
    spread = jnp.concatenate([twice] * (STATE_WIDTH // LANES), axis=1)
    return split_two(jnp.where(row // GROUP == column // STATES, spread * scale, 0.0))


def put_pair(ref, rows, re, im):
    ref[rows, :STATE_WIDTH] = re
    ref[rows, STATE_WIDTH:] = im


def put_split(ref, maps, scales):
    for part in range(2):
        columns = slice(part * STATE_WIDTH, (part + 1) * STATE_WIDTH)
        high, low = block_diagonal(maps[part], scales[part])
        ref[0, :, columns] = high
        ref[1, :, columns] = low


ALL = slice(None)


def prelude_kernel(extra, decay, cosine, sine, in_scale, in_map, trans, in_split):
    real, imag = wide_transitions(extra[...], decay[...], cosine[...], sine[...])
    put_pair(trans, slice(0, ROWS), real, imag)
    ends = running_products(real, imag, lambda rows, re, im: None)
    put_pair(trans, slice(ROWS, ROWS + SUBS), *ends)
    scale = flat_rows(in_scale[...])
    put_split(in_split, in_map, (scale, scale))


def fan_kernel(one, out):
    for i in range(out.shape[0]):
        out[i] = one[...]


def scan_blocks(inject, trans, last, store):
    run_re, run_im = inject[:SUBS, :STATE_WIDTH], inject[:SUBS, STATE_WIDTH:]
    store(slice(0, SUBS), run_re, run_im)
    for step in range(1, STEPS):
        rows = slice(step * SUBS, (step + 1) * SUBS)
        tr, ti = trans[rows, :STATE_WIDTH], trans[rows, STATE_WIDTH:]
        run_re, run_im = (
            tr * run_re - ti * run_im + inject[rows, :STATE_WIDTH],
            tr * run_im + ti * run_re + inject[rows, STATE_WIDTH:],
        )
        store(rows, run_re, run_im)
    last_re, last_im = last
    add = (jnp.zeros((1, STATE_WIDTH), f32), jnp.zeros((1, STATE_WIDTH), f32))
    mult = (jnp.ones((1, STATE_WIDTH), f32), jnp.zeros((1, STATE_WIDTH), f32))
    starts = []
    for sub in range(SUBS):
        starts.append((*mult, *add))
        one = slice(sub, sub + 1)
        tr, ti = last_re[one], last_im[one]
        add = (
            tr * add[0] - ti * add[1] + run_re[one],
            tr * add[1] + ti * add[0] + run_im[one],
        )
        mult = (tr * mult[0] - ti * mult[1], tr * mult[1] + ti * mult[0])
    return starts, (*mult, *add)


def inject_of(drive, in_split):
    return dot(drive, in_split[0]) + dot(drive, in_split[1])


def project_kernel(
    place,
    tokens,
    w_query,
    gain_far,
    w_key_far,
    tables_far,
    w_state_far,
    split_far,
    trans_far,
    w_value_far,
    keep,
    send,
    drive_far,
    gain,
    w_key,
    tables,
    w_state,
    in_split,
    trans,
    w_value,
    drive_near,
    arrived,
):
    far = (gain_far, w_state_far, split_far, tables_far, trans_far, w_key_far, w_value_far)
    near = (gain, w_state, in_split, tables, trans, w_key, w_value)
    copies = [
        pltpu.make_async_copy(source, target, arrived.at[i])
        for i, (source, target) in enumerate(zip(far, near))
    ]
    for copy in copies:
        copy.start()
    head = place[1]
    wide = tokens[...].astype(f32)
    scale = lax.rsqrt(jnp.mean(wide * wide, axis=-1, keepdims=True) + EPSILON)
    copies[0].wait()
    normed = (wide * scale * gain[...]).astype(bf16)

    def put(at, first, second):
        place_rows = slice(at * ROWS, (at + 1) * ROWS)
        keep[place_rows, :] = jnp.where(head == 0, first, second)
        send[place_rows, :] = jnp.where(head == 0, second, first)

    query = dot(normed, w_query[...])
    for copy in copies[1:4]:
        copy.wait()
    lane = lax.broadcasted_iota(jnp.int32, (ROWS, LANES), 1)
    first_half = lane % QK_DIM < QK_DIM // 2
    cos, sin = tables[0], tables[1]

    def turned(half):
        other = jnp.where(
            first_half,
            pltpu.roll(half, LANES - QK_DIM // 2, 1),
            pltpu.roll(half, QK_DIM // 2, 1),
        )
        return (half * cos + other * sin).astype(bf16)

    drive = dot(normed, w_state[...]).astype(bf16)
    ordered = dot(row_order(False).astype(bf16), drive).astype(bf16)
    drive_near[...] = ordered
    put(
        2,
        turned(query[:, :LANES]) * QK_DIM**-0.5,
        turned(query[:, LANES:]) * QK_DIM**-0.5,
    )
    for copy in copies[4:]:
        copy.wait()
    leaving = pltpu.make_async_copy(drive_near, drive_far, arrived.at[7])
    leaving.start()
    inject = inject_of(ordered, in_split)
    key = dot(normed, w_key[...])
    value = dot(normed, w_value[...])
    put(1, value[:, :LANES].astype(bf16), value[:, LANES:].astype(bf16))
    put(0, turned(key[:, :LANES]), turned(key[:, LANES:]))
    _, element_parts = scan_blocks(
        inject,
        trans,
        (trans[ROWS:, :STATE_WIDTH], trans[ROWS:, STATE_WIDTH:]),
        lambda where, re, im: None,
    )
    pieces = [
        member[:, tile * LANES : (tile + 1) * LANES]
        for member in element_parts
        for tile in range(STATE_WIDTH // LANES)
    ]
    element = jnp.concatenate(pieces, axis=0).astype(bf16)
    keep[3 * ROWS :, :] = element
    send[3 * ROWS :, :] = element
    leaving.wait()


def join_kernel(keep, got, out):
    for part in range(2):
        rows = slice(part * ROWS, (part + 1) * ROWS)
        out[2 * part * ROWS : (2 * part + 1) * ROWS, :] = keep[rows, :]
        out[(2 * part + 1) * ROWS : 2 * (part + 1) * ROWS, :] = got[rows, :]
    out[4 * ROWS : 4 * ROWS + EL_ROWS, :] = keep[3 * ROWS :, :]
    out[4 * ROWS + EL_ROWS :, :] = got[3 * ROWS :, :]


def attention_kernel(place, mix, sub_gain, keep, got, *rest):
    passed = rest[: RING - 1]
    out_keep, out_send, elements, scores, peak, total, numerator = rest[RING - 1 :]
    depth, head = place[0], place[1]
    pair = 2 * ROWS
    for k in range(RING - 1):
        elements[2 * EL_ROWS * k : 2 * EL_ROWS * (k + 1), :] = passed[k][2 * pair :, :]
    query = jnp.concatenate([keep[2 * ROWS : 3 * ROWS, :], got[2 * ROWS : 3 * ROWS, :]], axis=0)
    queries = (query[:, :QK_DIM], query[:, QK_DIM:])
    row = lax.broadcasted_iota(jnp.int32, (pair, pair), 0)
    column = lax.broadcasted_iota(jnp.int32, (pair, pair), 1)

    def segment(index):
        block = jnp.where(index < ROWS, head, 1 - head)
        return block * (ROWS // SEGMENT) + index % ROWS // SEGMENT

    allowed = segment(column) <= segment(row)
    own_key = jnp.concatenate([keep[:ROWS, :], got[:ROWS, :]], axis=0)
    own_value = jnp.concatenate([keep[ROWS:pair, :], got[ROWS:pair, :]], axis=0)
    for c in range(2):
        raw = dot_nt(queries[c], own_key[:, c * QK_DIM : (c + 1) * QK_DIM])
        masked = jnp.where(allowed, raw, MASK_FLOOR)
        scores[c, 0] = masked
        peak[c] = jnp.maximum(masked[:, :LANES], masked[:, LANES:])
    for k in range(1, RING):

        @pl.when(k <= depth)
        def _():
            for c in range(2):
                keys = passed[k - 1][:pair, c * QK_DIM : (c + 1) * QK_DIM]
                raw = dot_nt(queries[c], keys)
                scores[c, k] = raw
                peak[c] = jnp.maximum(peak[c], jnp.maximum(raw[:, :LANES], raw[:, LANES:]))

    tops = [jnp.max(peak[c], axis=-1, keepdims=True) for c in range(2)]
    for c in range(2):
        weight = jnp.exp(scores[c, 0] - tops[c])
        total[c] = weight[:, :LANES] + weight[:, LANES:]
        numerator[c] = dot(weight.astype(bf16), own_value)
    for k in range(1, RING):

        @pl.when(k <= depth)
        def _():
            for c in range(2):
                weight = jnp.exp(scores[c, k] - tops[c])
                total[c] += weight[:, :LANES] + weight[:, LANES:]
                numerator[c] += dot(weight.astype(bf16), passed[k - 1][pair : 2 * pair, :])

    mapped = [numerator[c] / jnp.sum(total[c], axis=-1, keepdims=True) for c in range(2)]
    difference = mapped[0] - mix[head] * mapped[1]
    mean = jnp.mean(difference * difference, axis=-1, keepdims=True)
    out = difference * lax.rsqrt(mean + EPSILON) * sub_gain[...] * (1.0 - LAMBDA_INIT)
    out_keep[...] = out[:ROWS].astype(bf16)
    out_send[...] = out[ROWS:].astype(bf16)


def state_kernel(
    place,
    init,
    got,
    elements,
    drive,
    skip,
    extra,
    decay,
    cosine,
    sine,
    in_scale,
    in_map,
    out_map,
    out,
    trans,
    product,
    in_split,
    out_split,
    states,
):
    depth, head, sequence = place[0], place[1], place[3]
    real, imag = wide_transitions(extra[...], decay[...], cosine[...], sine[...])
    put_pair(trans, ALL, real, imag)
    last = running_products(real, imag, lambda rows, re, im: put_pair(product, rows, re, im))
    scale = flat_rows(in_scale[...])
    put_split(in_split, in_map, (scale, scale))
    put_split(out_split, out_map, (1.0, -1.0))
    run_re, run_im = flat_rows(init[sequence, 0]), flat_rows(init[sequence, 1])

    def member(ref, base, index):
        tiles = STATE_WIDTH // LANES
        rows = [ref[base + index * tiles + t : base + index * tiles + t + 1, :] for t in range(tiles)]
        return jnp.concatenate(rows, axis=1).astype(f32)

    def advance(carry, ref, base, use):
        re, im = carry
        mr, mi, ar, ai = [member(ref, base, i) for i in range(4)]
        new_re, new_im = mr * re - mi * im + ar, mr * im + mi * re + ai
        return jnp.where(use, new_re, re), jnp.where(use, new_im, im)

    carry = (run_re, run_im)
    for k in range(RING - 1, 0, -1):
        use = k <= depth
        base = 2 * EL_ROWS * (k - 1)
        mine = [member(elements, base, i) for i in range(4)]
        other = [member(elements, base + EL_ROWS, i) for i in range(4)]
        early = [jnp.where(head == 0, a, b) for a, b in zip(mine, other)]
        late = [jnp.where(head == 0, b, a) for a, b in zip(mine, other)]
        for mr, mi, ar, ai in (early, late):
            re, im = carry
            new_re, new_im = mr * re - mi * im + ar, mr * im + mi * re + ai
            carry = jnp.where(use, new_re, re), jnp.where(use, new_im, im)
    carry = advance(carry, got, 3 * ROWS, head == 1)
    in_re, in_im = carry
    starts, _ = scan_blocks(
        inject_of(drive[...], in_split),
        trans,
        last,
        lambda rows, re, im: put_pair(states, rows, re, im),
    )
    add_re = jnp.concatenate([ar + mr * in_re - mi * in_im for mr, mi, ar, ai in starts], axis=0)
    add_im = jnp.concatenate([ai + mr * in_im + mi * in_re for mr, mi, ar, ai in starts], axis=0)
    for step in range(STEPS):
        rows = slice(step * SUBS, (step + 1) * SUBS)
        mr, mi = product[rows, :STATE_WIDTH], product[rows, STATE_WIDTH:]
        states[rows, :STATE_WIDTH] += mr * add_re - mi * add_im
        states[rows, STATE_WIDTH:] += mr * add_im + mi * add_re
    high, low = split_two(states[...])
    lane = lax.broadcasted_iota(jnp.int32, (GROUP, LANES), 1)
    spread = (lane % GROUP == lax.broadcasted_iota(jnp.int32, (GROUP, LANES), 0)).astype(f32)
    tiled = jnp.dot(
        skip[...], spread, precision=lax.Precision.HIGHEST, preferred_element_type=f32
    )
    own = lax.broadcasted_iota(jnp.int32, (GROUPS, LANES), 1) // GROUP
    own = own == lax.broadcasted_iota(jnp.int32, (GROUPS, LANES), 0)
    skip_row = jnp.sum(jnp.where(own, tiled, 0.0), axis=0, keepdims=True)
    mixed = (
        dot_nt(high, out_split[0])
        + dot_nt(low, out_split[0])
        + dot_nt(high, out_split[1])
        + skip_row * drive[...].astype(f32)
    )
    result = jax.nn.gelu(mixed).astype(bf16)
    out[...] = dot(row_order(True).astype(bf16), result).astype(bf16)


def output_kernel(place, state, kept, came, own, swapped_in, out, full):
    first = place[1] == 0
    mine, other = kept[...], came[...]
    acts = jnp.concatenate(
        [state[...], jnp.where(first, mine, other), jnp.where(first, other, mine)], axis=1
    )
    low_core = place[2] == 0
    for block in range(own.shape[0]):
        here, there = own[block], swapped_in[block]
        at = block % RING * 8 + block // RING
        full[at, 0] = jnp.where(low_core, here, there)
        full[at, 1] = jnp.where(low_core, there, here)
    weights = full[...].reshape(2 * own.shape[0] * own.shape[1], own.shape[2])
    out[...] = dot_nt(acts, weights).astype(bf16)


VMEM = pl.BlockSpec(memory_space=pltpu.VMEM)
SMEM = pl.BlockSpec(memory_space=pltpu.SMEM)
FAR = pl.BlockSpec(memory_space=pltpu.HBM)


def call(body, out_shapes, smem, args, scratch=(), far=0, far_out=0):
    near = len(args) - far
    specs = [SMEM if i in smem else VMEM if i < near else FAR for i in range(len(args))]
    return pl.pallas_call(
        body,
        out_shape=[jax.ShapeDtypeStruct(s, d) for s, d in out_shapes],
        in_specs=specs,
        out_specs=[VMEM] * (len(out_shapes) - far_out) + [FAR] * far_out,
        scratch_shapes=list(scratch),
        compiler_params=pltpu.CompilerParams(vmem_limit_bytes=20 * 1024 * 1024),
    )(*args)


def fanned(x, axis):
    shape = (lax.axis_size(axis), *x.shape)
    (copies,) = call(fan_kernel, [(shape, x.dtype)], (), (x,))
    return copies


def in_hbm(x):
    return pltpu.with_memory_space_constraint(x, pltpu.HBM)


def swapped(x, axis):
    return lax.ppermute(x, axis, [(0, 1), (1, 0)])


def local(
    tokens,
    norm_gain,
    w_query,
    w_key,
    w_value,
    w_state_in,
    decay_rate,
    rotation,
    extra_decay,
    in_map,
    out_map,
    skip_gain,
    init_state,
    mix_lambda,
    sub_gain,
    w_out_state,
    w_out_attn,
):
    depth, head, core = lax.axis_index("z"), lax.axis_index("h"), lax.axis_index("c")
    sequence = lax.axis_index("q") * 2 + core
    place = jnp.stack([depth, head, core, sequence]).astype(jnp.int32)
    gathered = lax.all_to_all(fanned(tokens, "tp"), "tp", 0, 0, tiled=True)
    weights = jnp.concatenate((w_out_state, w_out_attn), axis=0).T
    fan_weights = fanned(weights, "z")
    gathered = gathered.reshape(ROWS, tokens.shape[1])

    positions = ((depth * 2 + head) * ROWS + jnp.arange(ROWS, dtype=jnp.int32)).astype(f32)
    lane = jnp.arange(LANES, dtype=jnp.int32)
    inverse = ROTARY_BASE ** (-2.0 * (lane % (QK_DIM // 2)).astype(f32) / QK_DIM)
    angles = positions[:, None] * inverse[None, :]
    cosine_table = jnp.cos(angles)
    sine_table = jnp.where(lane % QK_DIM < QK_DIM // 2, -1.0, 1.0)[None, :] * jnp.sin(angles)
    maps = (2, GROUPS * GROUP, STATES)
    wide = ((ROWS, 2 * STATE_WIDTH), f32)
    diagonal = ((2, GROUPS * GROUP, 2 * STATE_WIDTH), bf16)
    state_params = (
        extra_decay,
        decay_rate,
        jnp.cos(rotation),
        jnp.sin(rotation),
        jnp.sqrt(-jnp.expm1(-2.0 * decay_rate)),
        jnp.swapaxes(in_map, 2, 3).reshape(maps),
    )
    tables = jnp.stack((cosine_table, sine_table))
    trans, in_split = call(
        prelude_kernel, [((ROWS + SUBS, 2 * STATE_WIDTH), f32), diagonal], (), state_params
    )

    fan_weights, gathered, trans, in_split, tables = lax.optimization_barrier(
        (fan_weights, gathered, trans, in_split, tables)
    )
    weight_rows = lax.all_to_all(fan_weights, "z", 0, 0, tiled=True)
    weight_rows = weight_rows.reshape(-1, weights.shape[1])

    payload = ((3 * ROWS + EL_ROWS, LANES), bf16)
    keep, send, drive = call(
        project_kernel,
        [payload, payload, ((ROWS, GROUPS * GROUP), bf16)],
        (0,),
        (
            place,
            gathered,
            w_query,
            in_hbm(norm_gain.reshape(1, -1)),
            in_hbm(w_key),
            in_hbm(tables),
            in_hbm(w_state_in),
            in_hbm(in_split),
            in_hbm(trans),
            in_hbm(w_value),
        ),
        [
            pltpu.VMEM((1, tokens.shape[1]), f32),
            pltpu.VMEM(w_key.shape, bf16),
            pltpu.VMEM(tables.shape, f32),
            pltpu.VMEM(w_state_in.shape, bf16),
            pltpu.VMEM(in_split.shape, bf16),
            pltpu.VMEM(trans.shape, f32),
            pltpu.VMEM(w_value.shape, bf16),
            pltpu.VMEM((ROWS, GROUPS * GROUP), bf16),
            pltpu.SemaphoreType.DMA((8,)),
        ],
        far=7,
        far_out=1,
    )
    got = swapped(send, "h")
    (shared,) = call(join_kernel, [((4 * ROWS + 2 * EL_ROWS, LANES), bf16)], (), (keep, got))

    def along(x, pairs):
        return lax.ppermute(x, "z", pairs)

    up = lambda by, first=0: [(i, i + by) for i in range(first, RING - by)]
    two = along(shared, up(2))
    six = along(shared, [(0, 6), (1, 7), (2, 0)])
    one = along(shared, up(1))
    seven = along(shared, [(0, 7)])
    four = along(two, up(2, 2))
    three = along(two, up(1, 2))
    five = along(six, [(6, 5), (7, 6), (0, 7)])
    passed = [one, two, three, four, five, six, seven]
    weight_blocks = lax.all_to_all(fanned(weight_rows, Y), Y, 0, 0, tiled=True)

    pair = (2, 2 * ROWS, LANES)
    out_keep, out_send, elements = call(
        attention_kernel,
        [((ROWS, LANES), bf16)] * 2 + [((2 * EL_ROWS * (RING - 1), LANES), bf16)],
        (0, 1),
        (place, mix_lambda, sub_gain.reshape(1, -1), keep, got, *passed),
        [pltpu.VMEM((2, RING, 2 * ROWS, 2 * ROWS), f32)] + [pltpu.VMEM(pair, f32)] * 3,
    )
    came = swapped(out_send, "h")

    (state_out,) = call(
        state_kernel,
        [((ROWS, GROUPS * GROUP), bf16)],
        (0,),
        (place, init_state, got, elements, drive, skip_gain, *state_params, out_map.reshape(maps)),
        [
            pltpu.VMEM(wide[0], f32),
            pltpu.VMEM(wide[0], f32),
            pltpu.VMEM(diagonal[0], bf16),
            pltpu.VMEM(diagonal[0], bf16),
            pltpu.VMEM(wide[0], f32),
        ],
    )

    other_blocks = swapped(weight_blocks, "c")
    width = w_out_attn.shape[1]
    blocks = (-1, width, weights.shape[1])

    (partial,) = call(
        output_kernel,
        [((ROWS, RING * 2 * 8 * width), bf16)],
        (0,),
        (
            place,
            state_out,
            out_keep,
            came,
            weight_blocks.reshape(blocks),
            other_blocks.reshape(blocks),
        ),
        [pltpu.VMEM((RING * 8, 2, width, weights.shape[1]), bf16)],
    )
    parts = partial.reshape(lax.axis_size("tp"), tokens.shape[0], -1)
    shares = lax.all_to_all(parts, "tp", 0, 0, tiled=True)
    return jnp.sum(shares.astype(f32), axis=0).astype(bf16)


def solution(mesh):
    split = Mesh(
        mesh.devices.reshape(8, 2, 4, 2, mesh.shape["tp"]), ("z", "h", "q", "c", "tp")
    )

    return jax.shard_map(
        local,
        mesh=split,
        in_specs=(
            P(SP_TP, None),
            P(),
            P(None, "tp"),
            P(None, "tp"),
            P(None, "tp"),
            P(None, "tp"),
            P("tp", None),
            P("tp", None),
            P(SP, "tp"),
            P(None, "tp", None, None),
            P(None, "tp", None, None),
            P("tp", None),
            P(None, None, "tp", None),
            P("tp"),
            P(),
            P("tp", SP),
            P("tp", SP),
        ),
        out_specs=P(SP_TP, None),
        check_vma=False,
    )
```

```python
import jax
import jax.numpy as jnp
from jax import lax
from jax.experimental import pallas as pl
from jax.experimental.pallas import tpu as pltpu
from jax.sharding import Mesh
from jax.sharding import PartitionSpec as P

SP = ("z", "h", "q", "c")
Y = ("h", "q")
SP_TP = ("z", "h", "q", "c", "tp")

EPSILON = 1e-06
ROTARY_BASE = 10000.0
LAMBDA_INIT = 0.2
MASK_FLOOR = -1e30
ROWS = 128
SUBS = 8
STEPS = ROWS // SUBS
LANES = 128
QK_DIM = 64
SEGMENT = 64
STATE_WIDTH = 512
GROUPS = 8
GROUP = 16
STATES = 64
EL_ROWS = 16
RING = 8


f32 = jnp.float32
bf16 = jnp.bfloat16


def dot(a, b):
    return jnp.dot(a, b, preferred_element_type=f32)


def dot_nt(a, b):
    return lax.dot_general(a, b, (((1,), (1,)), ((), ())), preferred_element_type=f32)


def split_two(x):
    high = x.astype(bf16)
    return high, (x - high.astype(f32)).astype(bf16)


def row_order(transposed):
    first = lax.broadcasted_iota(jnp.int32, (ROWS, ROWS), 0)
    second = lax.broadcasted_iota(jnp.int32, (ROWS, ROWS), 1)
    row, token = (second, first) if transposed else (first, second)
    return (row % SUBS) * STEPS + row // SUBS == token


def flat_rows(x):
    twice = jnp.concatenate([x, x], axis=1)
    low = lax.broadcasted_iota(jnp.int32, (1, LANES), 1) < STATES
    tiles = [
        jnp.where(low, twice[2 * t : 2 * t + 1], twice[2 * t + 1 : 2 * t + 2])
        for t in range(GROUPS // 2)
    ]
    return jnp.concatenate(tiles, axis=1)


def wide_transitions(extra, decay, cosine, sine):
    group = lax.broadcasted_iota(jnp.int32, (GROUPS, STATE_WIDTH), 0)
    lane = lax.broadcasted_iota(jnp.int32, (GROUPS, STATE_WIDTH), 1)
    widen = (lane // STATES == group).astype(f32)
    highest = lax.Precision.HIGHEST
    ordered = jnp.dot(
        row_order(False).astype(f32), extra, precision=highest, preferred_element_type=f32
    )
    wide = jnp.dot(ordered, widen, precision=highest, preferred_element_type=f32)
    magnitude = jnp.exp(wide - flat_rows(decay))
    return magnitude * flat_rows(cosine), magnitude * flat_rows(sine)


def running_products(real, imag, store):
    run_re, run_im = real[:SUBS], imag[:SUBS]
    store(slice(0, SUBS), run_re, run_im)
    for step in range(1, STEPS):
        rows = slice(step * SUBS, (step + 1) * SUBS)
        tr, ti = real[rows], imag[rows]
        run_re, run_im = tr * run_re - ti * run_im, tr * run_im + ti * run_re
        store(rows, run_re, run_im)
    return run_re, run_im


def block_diagonal(compact, scale):
    row = lax.broadcasted_iota(jnp.int32, (GROUPS * GROUP, STATE_WIDTH), 0)
    column = lax.broadcasted_iota(jnp.int32, (GROUPS * GROUP, STATE_WIDTH), 1)
    twice = jnp.concatenate([compact, compact], axis=1)
    spread = jnp.concatenate([twice] * (STATE_WIDTH // LANES), axis=1)
    return split_two(jnp.where(row // GROUP == column // STATES, spread * scale, 0.0))


def put_pair(ref, rows, re, im):
    ref[rows, :STATE_WIDTH] = re
    ref[rows, STATE_WIDTH:] = im


def put_split(ref, maps, scales):
    for part in range(2):
        columns = slice(part * STATE_WIDTH, (part + 1) * STATE_WIDTH)
        high, low = block_diagonal(maps[part], scales[part])
        ref[0, :, columns] = high
        ref[1, :, columns] = low


ALL = slice(None)


def prelude_kernel(extra, decay, cosine, sine, in_scale, in_map, trans, in_split):
    real, imag = wide_transitions(extra[...], decay[...], cosine[...], sine[...])
    put_pair(trans, slice(0, ROWS), real, imag)
    ends = running_products(real, imag, lambda rows, re, im: None)
    put_pair(trans, slice(ROWS, ROWS + SUBS), *ends)
    scale = flat_rows(in_scale[...])
    put_split(in_split, in_map, (scale, scale))


def fan_kernel(one, out):
    for i in range(out.shape[0]):
        out[i] = one[...]


def scan_blocks(inject, trans, last, store):
    run_re, run_im = inject[:SUBS, :STATE_WIDTH], inject[:SUBS, STATE_WIDTH:]
    store(slice(0, SUBS), run_re, run_im)
    for step in range(1, STEPS):
        rows = slice(step * SUBS, (step + 1) * SUBS)
        tr, ti = trans[rows, :STATE_WIDTH], trans[rows, STATE_WIDTH:]
        run_re, run_im = (
            tr * run_re - ti * run_im + inject[rows, :STATE_WIDTH],
            tr * run_im + ti * run_re + inject[rows, STATE_WIDTH:],
        )
        store(rows, run_re, run_im)
    last_re, last_im = last
    add = (jnp.zeros((1, STATE_WIDTH), f32), jnp.zeros((1, STATE_WIDTH), f32))
    mult = (jnp.ones((1, STATE_WIDTH), f32), jnp.zeros((1, STATE_WIDTH), f32))
    starts = []
    for sub in range(SUBS):
        starts.append((*mult, *add))
        one = slice(sub, sub + 1)
        tr, ti = last_re[one], last_im[one]
        add = (
            tr * add[0] - ti * add[1] + run_re[one],
            tr * add[1] + ti * add[0] + run_im[one],
        )
        mult = (tr * mult[0] - ti * mult[1], tr * mult[1] + ti * mult[0])
    return starts, (*mult, *add)


def inject_of(drive, in_split):
    return dot(drive, in_split[0]) + dot(drive, in_split[1])


def project_kernel(
    place,
    tokens,
    w_query,
    gain_far,
    w_key_far,
    tables_far,
    w_state_far,
    split_far,
    trans_far,
    w_value_far,
    keep,
    send,
    drive_far,
    gain,
    w_key,
    tables,
    w_state,
    in_split,
    trans,
    w_value,
    drive_near,
    arrived,
):
    far = (gain_far, w_state_far, split_far, tables_far, trans_far, w_key_far, w_value_far)
    near = (gain, w_state, in_split, tables, trans, w_key, w_value)
    copies = [
        pltpu.make_async_copy(source, target, arrived.at[i])
        for i, (source, target) in enumerate(zip(far, near))
    ]
    for copy in copies:
        copy.start()
    head = place[1]
    wide = tokens[...].astype(f32)
    scale = lax.rsqrt(jnp.mean(wide * wide, axis=-1, keepdims=True) + EPSILON)
    copies[0].wait()
    normed = (wide * scale * gain[...]).astype(bf16)

    def put(at, first, second):
        place_rows = slice(at * ROWS, (at + 1) * ROWS)
        keep[place_rows, :] = jnp.where(head == 0, first, second)
        send[place_rows, :] = jnp.where(head == 0, second, first)

    query = dot(normed, w_query[...])
    for copy in copies[1:4]:
        copy.wait()
    lane = lax.broadcasted_iota(jnp.int32, (ROWS, LANES), 1)
    first_half = lane % QK_DIM < QK_DIM // 2
    cos, sin = tables[0], tables[1]

    def turned(half):
        other = jnp.where(
            first_half,
            pltpu.roll(half, LANES - QK_DIM // 2, 1),
            pltpu.roll(half, QK_DIM // 2, 1),
        )
        return (half * cos + other * sin).astype(bf16)

    drive = dot(normed, w_state[...]).astype(bf16)
    ordered = dot(row_order(False).astype(bf16), drive).astype(bf16)
    drive_near[...] = ordered
    put(
        2,
        turned(query[:, :LANES]) * QK_DIM**-0.5,
        turned(query[:, LANES:]) * QK_DIM**-0.5,
    )
    for copy in copies[4:]:
        copy.wait()
    leaving = pltpu.make_async_copy(drive_near, drive_far, arrived.at[7])
    leaving.start()
    inject = inject_of(ordered, in_split)
    key = dot(normed, w_key[...])
    value = dot(normed, w_value[...])
    put(1, value[:, :LANES].astype(bf16), value[:, LANES:].astype(bf16))
    put(0, turned(key[:, :LANES]), turned(key[:, LANES:]))
    _, element_parts = scan_blocks(
        inject,
        trans,
        (trans[ROWS:, :STATE_WIDTH], trans[ROWS:, STATE_WIDTH:]),
        lambda where, re, im: None,
    )
    pieces = [
        member[:, tile * LANES : (tile + 1) * LANES]
        for member in element_parts
        for tile in range(STATE_WIDTH // LANES)
    ]
    element = jnp.concatenate(pieces, axis=0).astype(bf16)
    keep[3 * ROWS :, :] = element
    send[3 * ROWS :, :] = element
    leaving.wait()


def join_kernel(keep, got, out):
    for part in range(2):
        rows = slice(part * ROWS, (part + 1) * ROWS)
        out[2 * part * ROWS : (2 * part + 1) * ROWS, :] = keep[rows, :]
        out[(2 * part + 1) * ROWS : 2 * (part + 1) * ROWS, :] = got[rows, :]
    out[4 * ROWS : 4 * ROWS + EL_ROWS, :] = keep[3 * ROWS :, :]
    out[4 * ROWS + EL_ROWS :, :] = got[3 * ROWS :, :]


def attention_kernel(place, mix, sub_gain, keep, got, *rest):
    passed = rest[: RING - 1]
    out_keep, out_send, elements, scores, peak, total, numerator = rest[RING - 1 :]
    depth, head = place[0], place[1]
    pair = 2 * ROWS
    for k in range(RING - 1):
        elements[2 * EL_ROWS * k : 2 * EL_ROWS * (k + 1), :] = passed[k][2 * pair :, :]
    query = jnp.concatenate([keep[2 * ROWS : 3 * ROWS, :], got[2 * ROWS : 3 * ROWS, :]], axis=0)
    low = lax.broadcasted_iota(jnp.int32, (pair, LANES), 1) < QK_DIM
    zero = jnp.zeros_like(query)
    both = jnp.concatenate([jnp.where(low, query, zero), jnp.where(low, zero, query)], axis=0)
    row = lax.broadcasted_iota(jnp.int32, (2 * pair, pair), 0) % pair
    column = lax.broadcasted_iota(jnp.int32, (2 * pair, pair), 1)

    def segment(index):
        block = jnp.where(index < ROWS, head, 1 - head)
        return block * (ROWS // SEGMENT) + index % ROWS // SEGMENT

    allowed = segment(column) <= segment(row)
    own_key = jnp.concatenate([keep[:ROWS, :], got[:ROWS, :]], axis=0)
    own_value = jnp.concatenate([keep[ROWS:pair, :], got[ROWS:pair, :]], axis=0)
    masked = jnp.where(allowed, dot_nt(both, own_key), MASK_FLOOR)
    scores[0] = masked
    peak[...] = jnp.maximum(masked[:, :LANES], masked[:, LANES:])
    for k in range(1, RING):

        @pl.when(k <= depth)
        def _():
            raw = dot_nt(both, passed[k - 1][:pair, :])
            scores[k] = raw
            peak[...] = jnp.maximum(peak[...], jnp.maximum(raw[:, :LANES], raw[:, LANES:]))

    top = jnp.max(peak[...], axis=-1, keepdims=True)
    weight = jnp.exp(scores[0] - top)
    total[...] = weight[:, :LANES] + weight[:, LANES:]
    numerator[...] = dot(weight.astype(bf16), own_value)
    for k in range(1, RING):

        @pl.when(k <= depth)
        def _():
            weight = jnp.exp(scores[k] - top)
            total[...] += weight[:, :LANES] + weight[:, LANES:]
            numerator[...] += dot(weight.astype(bf16), passed[k - 1][pair : 2 * pair, :])

    mapped = numerator[...] / jnp.sum(total[...], axis=-1, keepdims=True)
    difference = mapped[:pair] - mix[head] * mapped[pair:]
    mean = jnp.mean(difference * difference, axis=-1, keepdims=True)
    out = difference * lax.rsqrt(mean + EPSILON) * sub_gain[...] * (1.0 - LAMBDA_INIT)
    out_keep[...] = out[:ROWS].astype(bf16)
    out_send[...] = out[ROWS:].astype(bf16)


def state_kernel(
    place,
    init,
    got,
    elements,
    drive,
    skip,
    extra,
    decay,
    cosine,
    sine,
    in_scale,
    in_map,
    out_map,
    out,
    trans,
    product,
    in_split,
    out_split,
    states,
):
    depth, head, sequence = place[0], place[1], place[3]
    real, imag = wide_transitions(extra[...], decay[...], cosine[...], sine[...])
    put_pair(trans, ALL, real, imag)
    last = running_products(real, imag, lambda rows, re, im: put_pair(product, rows, re, im))
    scale = flat_rows(in_scale[...])
    put_split(in_split, in_map, (scale, scale))
    put_split(out_split, out_map, (1.0, -1.0))
    run_re, run_im = flat_rows(init[sequence, 0]), flat_rows(init[sequence, 1])

    def member(ref, base, index):
        tiles = STATE_WIDTH // LANES
        rows = [ref[base + index * tiles + t : base + index * tiles + t + 1, :] for t in range(tiles)]
        return jnp.concatenate(rows, axis=1).astype(f32)

    def advance(carry, ref, base, use):
        re, im = carry
        mr, mi, ar, ai = [member(ref, base, i) for i in range(4)]
        new_re, new_im = mr * re - mi * im + ar, mr * im + mi * re + ai
        return jnp.where(use, new_re, re), jnp.where(use, new_im, im)

    carry = (run_re, run_im)
    for k in range(RING - 1, 0, -1):
        use = k <= depth
        base = 2 * EL_ROWS * (k - 1)
        mine = [member(elements, base, i) for i in range(4)]
        other = [member(elements, base + EL_ROWS, i) for i in range(4)]
        early = [jnp.where(head == 0, a, b) for a, b in zip(mine, other)]
        late = [jnp.where(head == 0, b, a) for a, b in zip(mine, other)]
        for mr, mi, ar, ai in (early, late):
            re, im = carry
            new_re, new_im = mr * re - mi * im + ar, mr * im + mi * re + ai
            carry = jnp.where(use, new_re, re), jnp.where(use, new_im, im)
    carry = advance(carry, got, 3 * ROWS, head == 1)
    in_re, in_im = carry
    starts, _ = scan_blocks(
        inject_of(drive[...], in_split),
        trans,
        last,
        lambda rows, re, im: put_pair(states, rows, re, im),
    )
    add_re = jnp.concatenate([ar + mr * in_re - mi * in_im for mr, mi, ar, ai in starts], axis=0)
    add_im = jnp.concatenate([ai + mr * in_im + mi * in_re for mr, mi, ar, ai in starts], axis=0)
    for step in range(STEPS):
        rows = slice(step * SUBS, (step + 1) * SUBS)
        mr, mi = product[rows, :STATE_WIDTH], product[rows, STATE_WIDTH:]
        states[rows, :STATE_WIDTH] += mr * add_re - mi * add_im
        states[rows, STATE_WIDTH:] += mr * add_im + mi * add_re
    high, low = split_two(states[...])
    lane = lax.broadcasted_iota(jnp.int32, (GROUP, LANES), 1)
    spread = (lane % GROUP == lax.broadcasted_iota(jnp.int32, (GROUP, LANES), 0)).astype(f32)
    tiled = jnp.dot(
        skip[...], spread, precision=lax.Precision.HIGHEST, preferred_element_type=f32
    )
    own = lax.broadcasted_iota(jnp.int32, (GROUPS, LANES), 1) // GROUP
    own = own == lax.broadcasted_iota(jnp.int32, (GROUPS, LANES), 0)
    skip_row = jnp.sum(jnp.where(own, tiled, 0.0), axis=0, keepdims=True)
    mixed = (
        dot_nt(high, out_split[0])
        + dot_nt(low, out_split[0])
        + dot_nt(high, out_split[1])
        + skip_row * drive[...].astype(f32)
    )
    result = jax.nn.gelu(mixed).astype(bf16)
    out[...] = dot(row_order(True).astype(bf16), result).astype(bf16)


def output_kernel(place, state, kept, came, own, swapped_in, out, full):
    first = place[1] == 0
    mine, other = kept[...], came[...]
    acts = jnp.concatenate(
        [state[...], jnp.where(first, mine, other), jnp.where(first, other, mine)], axis=1
    )
    low_core = place[2] == 0
    for block in range(own.shape[0]):
        here, there = own[block], swapped_in[block]
        at = block % RING * 8 + block // RING
        full[at, 0] = jnp.where(low_core, here, there)
        full[at, 1] = jnp.where(low_core, there, here)
    weights = full[...].reshape(2 * own.shape[0] * own.shape[1], own.shape[2])
    out[...] = dot_nt(acts, weights).astype(bf16)


VMEM = pl.BlockSpec(memory_space=pltpu.VMEM)
SMEM = pl.BlockSpec(memory_space=pltpu.SMEM)
FAR = pl.BlockSpec(memory_space=pltpu.HBM)


def call(body, out_shapes, smem, args, scratch=(), far=0, far_out=0):
    near = len(args) - far
    specs = [SMEM if i in smem else VMEM if i < near else FAR for i in range(len(args))]
    return pl.pallas_call(
        body,
        out_shape=[jax.ShapeDtypeStruct(s, d) for s, d in out_shapes],
        in_specs=specs,
        out_specs=[VMEM] * (len(out_shapes) - far_out) + [FAR] * far_out,
        scratch_shapes=list(scratch),
        compiler_params=pltpu.CompilerParams(vmem_limit_bytes=20 * 1024 * 1024),
    )(*args)


def fanned(x, axis):
    shape = (lax.axis_size(axis), *x.shape)
    (copies,) = call(fan_kernel, [(shape, x.dtype)], (), (x,))
    return copies


def in_hbm(x):
    return pltpu.with_memory_space_constraint(x, pltpu.HBM)


def swapped(x, axis):
    return lax.ppermute(x, axis, [(0, 1), (1, 0)])


def local(
    tokens,
    norm_gain,
    w_query,
    w_key,
    w_value,
    w_state_in,
    decay_rate,
    rotation,
    extra_decay,
    in_map,
    out_map,
    skip_gain,
    init_state,
    mix_lambda,
    sub_gain,
    w_out_state,
    w_out_attn,
):
    depth, head, core = lax.axis_index("z"), lax.axis_index("h"), lax.axis_index("c")
    sequence = lax.axis_index("q") * 2 + core
    place = jnp.stack([depth, head, core, sequence]).astype(jnp.int32)
    gathered = lax.all_to_all(fanned(tokens, "tp"), "tp", 0, 0, tiled=True)
    weights = jnp.concatenate((w_out_state, w_out_attn), axis=0).T
    fan_weights = fanned(weights, "z")
    gathered = gathered.reshape(ROWS, tokens.shape[1])

    positions = ((depth * 2 + head) * ROWS + jnp.arange(ROWS, dtype=jnp.int32)).astype(f32)
    lane = jnp.arange(LANES, dtype=jnp.int32)
    inverse = ROTARY_BASE ** (-2.0 * (lane % (QK_DIM // 2)).astype(f32) / QK_DIM)
    angles = positions[:, None] * inverse[None, :]
    cosine_table = jnp.cos(angles)
    sine_table = jnp.where(lane % QK_DIM < QK_DIM // 2, -1.0, 1.0)[None, :] * jnp.sin(angles)
    maps = (2, GROUPS * GROUP, STATES)
    wide = ((ROWS, 2 * STATE_WIDTH), f32)
    diagonal = ((2, GROUPS * GROUP, 2 * STATE_WIDTH), bf16)
    state_params = (
        extra_decay,
        decay_rate,
        jnp.cos(rotation),
        jnp.sin(rotation),
        jnp.sqrt(-jnp.expm1(-2.0 * decay_rate)),
        jnp.swapaxes(in_map, 2, 3).reshape(maps),
    )
    tables = jnp.stack((cosine_table, sine_table))
    trans, in_split = call(
        prelude_kernel, [((ROWS + SUBS, 2 * STATE_WIDTH), f32), diagonal], (), state_params
    )

    fan_weights, gathered, trans, in_split, tables = lax.optimization_barrier(
        (fan_weights, gathered, trans, in_split, tables)
    )
    weight_rows = lax.all_to_all(fan_weights, "z", 0, 0, tiled=True)
    weight_rows = weight_rows.reshape(-1, weights.shape[1])

    payload = ((3 * ROWS + EL_ROWS, LANES), bf16)
    keep, send, drive = call(
        project_kernel,
        [payload, payload, ((ROWS, GROUPS * GROUP), bf16)],
        (0,),
        (
            place,
            gathered,
            w_query,
            in_hbm(norm_gain.reshape(1, -1)),
            in_hbm(w_key),
            in_hbm(tables),
            in_hbm(w_state_in),
            in_hbm(in_split),
            in_hbm(trans),
            in_hbm(w_value),
        ),
        [
            pltpu.VMEM((1, tokens.shape[1]), f32),
            pltpu.VMEM(w_key.shape, bf16),
            pltpu.VMEM(tables.shape, f32),
            pltpu.VMEM(w_state_in.shape, bf16),
            pltpu.VMEM(in_split.shape, bf16),
            pltpu.VMEM(trans.shape, f32),
            pltpu.VMEM(w_value.shape, bf16),
            pltpu.VMEM((ROWS, GROUPS * GROUP), bf16),
            pltpu.SemaphoreType.DMA((8,)),
        ],
        far=7,
        far_out=1,
    )
    got = swapped(send, "h")
    (shared,) = call(join_kernel, [((4 * ROWS + 2 * EL_ROWS, LANES), bf16)], (), (keep, got))

    def along(x, pairs):
        return lax.ppermute(x, "z", pairs)

    up = lambda by, first=0: [(i, i + by) for i in range(first, RING - by)]
    two = along(shared, up(2))
    six = along(shared, [(0, 6), (1, 7), (2, 0)])
    one = along(shared, up(1))
    seven = along(shared, [(0, 7)])
    four = along(two, up(2, 2))
    three = along(two, up(1, 2))
    five = along(six, [(6, 5), (7, 6), (0, 7)])
    passed = [one, two, three, four, five, six, seven]
    weight_blocks = lax.all_to_all(fanned(weight_rows, Y), Y, 0, 0, tiled=True)

    pair = (4 * ROWS, LANES)
    out_keep, out_send, elements = call(
        attention_kernel,
        [((ROWS, LANES), bf16)] * 2 + [((2 * EL_ROWS * (RING - 1), LANES), bf16)],
        (0, 1),
        (place, mix_lambda, sub_gain.reshape(1, -1), keep, got, *passed),
        [pltpu.VMEM((RING, 4 * ROWS, 2 * ROWS), f32)] + [pltpu.VMEM(pair, f32)] * 3,
    )
    came = swapped(out_send, "h")

    (state_out,) = call(
        state_kernel,
        [((ROWS, GROUPS * GROUP), bf16)],
        (0,),
        (place, init_state, got, elements, drive, skip_gain, *state_params, out_map.reshape(maps)),
        [
            pltpu.VMEM(wide[0], f32),
            pltpu.VMEM(wide[0], f32),
            pltpu.VMEM(diagonal[0], bf16),
            pltpu.VMEM(diagonal[0], bf16),
            pltpu.VMEM(wide[0], f32),
        ],
    )

    other_blocks = swapped(weight_blocks, "c")
    width = w_out_attn.shape[1]
    blocks = (-1, width, weights.shape[1])

    (partial,) = call(
        output_kernel,
        [((ROWS, RING * 2 * 8 * width), bf16)],
        (0,),
        (
            place,
            state_out,
            out_keep,
            came,
            weight_blocks.reshape(blocks),
            other_blocks.reshape(blocks),
        ),
        [pltpu.VMEM((RING * 8, 2, width, weights.shape[1]), bf16)],
    )
    parts = partial.reshape(lax.axis_size("tp"), tokens.shape[0], -1)
    shares = lax.all_to_all(parts, "tp", 0, 0, tiled=True)
    return jnp.sum(shares.astype(f32), axis=0).astype(bf16)


def solution(mesh):
    split = Mesh(
        mesh.devices.reshape(8, 2, 4, 2, mesh.shape["tp"]), ("z", "h", "q", "c", "tp")
    )

    return jax.shard_map(
        local,
        mesh=split,
        in_specs=(
            P(SP_TP, None),
            P(),
            P(None, "tp"),
            P(None, "tp"),
            P(None, "tp"),
            P(None, "tp"),
            P("tp", None),
            P("tp", None),
            P(SP, "tp"),
            P(None, "tp", None, None),
            P(None, "tp", None, None),
            P("tp", None),
            P(None, None, "tp", None),
            P("tp"),
            P(),
            P("tp", SP),
            P("tp", SP),
        ),
        out_specs=P(SP_TP, None),
        check_vma=False,
    )
```

```python
import jax
import jax.numpy as jnp
from jax import lax
from jax.experimental import pallas as pl
from jax.experimental.pallas import tpu as pltpu
from jax.sharding import Mesh
from jax.sharding import PartitionSpec as P

SP = ("z", "h", "q", "c")
Y = ("h", "q")
SP_TP = ("z", "h", "q", "c", "tp")

EPSILON = 1e-06
ROTARY_BASE = 10000.0
LAMBDA_INIT = 0.2
MASK_FLOOR = -1e30
ROWS = 128
SUBS = 8
STEPS = ROWS // SUBS
LANES = 128
QK_DIM = 64
SEGMENT = 64
STATE_WIDTH = 512
GROUPS = 8
GROUP = 16
STATES = 64
EL_ROWS = 16
RING = 8


f32 = jnp.float32
bf16 = jnp.bfloat16


def dot(a, b):
    return jnp.dot(a, b, preferred_element_type=f32)


def dot_nt(a, b):
    return lax.dot_general(a, b, (((1,), (1,)), ((), ())), preferred_element_type=f32)


def split_two(x):
    high = x.astype(bf16)
    return high, (x - high.astype(f32)).astype(bf16)


def row_order(transposed):
    first = lax.broadcasted_iota(jnp.int32, (ROWS, ROWS), 0)
    second = lax.broadcasted_iota(jnp.int32, (ROWS, ROWS), 1)
    row, token = (second, first) if transposed else (first, second)
    return (row % SUBS) * STEPS + row // SUBS == token


def flat_rows(x):
    twice = jnp.concatenate([x, x], axis=1)
    low = lax.broadcasted_iota(jnp.int32, (1, LANES), 1) < STATES
    tiles = [
        jnp.where(low, twice[2 * t : 2 * t + 1], twice[2 * t + 1 : 2 * t + 2])
        for t in range(GROUPS // 2)
    ]
    return jnp.concatenate(tiles, axis=1)


def wide_transitions(extra, decay, cosine, sine):
    group = lax.broadcasted_iota(jnp.int32, (GROUPS, STATE_WIDTH), 0)
    lane = lax.broadcasted_iota(jnp.int32, (GROUPS, STATE_WIDTH), 1)
    widen = (lane // STATES == group).astype(f32)
    highest = lax.Precision.HIGHEST
    ordered = jnp.dot(
        row_order(False).astype(f32), extra, precision=highest, preferred_element_type=f32
    )
    wide = jnp.dot(ordered, widen, precision=highest, preferred_element_type=f32)
    magnitude = jnp.exp(wide - flat_rows(decay))
    return magnitude * flat_rows(cosine), magnitude * flat_rows(sine)


def running_products(real, imag, store):
    run_re, run_im = real[:SUBS], imag[:SUBS]
    store(slice(0, SUBS), run_re, run_im)
    for step in range(1, STEPS):
        rows = slice(step * SUBS, (step + 1) * SUBS)
        tr, ti = real[rows], imag[rows]
        run_re, run_im = tr * run_re - ti * run_im, tr * run_im + ti * run_re
        store(rows, run_re, run_im)
    return run_re, run_im


def block_diagonal(compact, scale):
    row = lax.broadcasted_iota(jnp.int32, (GROUPS * GROUP, STATE_WIDTH), 0)
    column = lax.broadcasted_iota(jnp.int32, (GROUPS * GROUP, STATE_WIDTH), 1)
    twice = jnp.concatenate([compact, compact], axis=1)
    spread = jnp.concatenate([twice] * (STATE_WIDTH // LANES), axis=1)
    return split_two(jnp.where(row // GROUP == column // STATES, spread * scale, 0.0))


def put_pair(ref, rows, re, im):
    ref[rows, :STATE_WIDTH] = re
    ref[rows, STATE_WIDTH:] = im


def put_split(ref, maps, scales):
    for part in range(2):
        columns = slice(part * STATE_WIDTH, (part + 1) * STATE_WIDTH)
        high, low = block_diagonal(maps[part], scales[part])
        ref[0, :, columns] = high
        ref[1, :, columns] = low


ALL = slice(None)


def prelude_kernel(extra, decay, cosine, sine, in_scale, in_map, trans, in_split):
    real, imag = wide_transitions(extra[...], decay[...], cosine[...], sine[...])
    put_pair(trans, slice(0, ROWS), real, imag)
    ends = running_products(real, imag, lambda rows, re, im: None)
    put_pair(trans, slice(ROWS, ROWS + SUBS), *ends)
    scale = flat_rows(in_scale[...])
    put_split(in_split, in_map, (scale, scale))


def fan_kernel(one, out):
    for i in range(out.shape[0]):
        out[i] = one[...]


def scan_blocks(inject, trans, last, store):
    run_re, run_im = inject[:SUBS, :STATE_WIDTH], inject[:SUBS, STATE_WIDTH:]
    store(slice(0, SUBS), run_re, run_im)
    for step in range(1, STEPS):
        rows = slice(step * SUBS, (step + 1) * SUBS)
        tr, ti = trans[rows, :STATE_WIDTH], trans[rows, STATE_WIDTH:]
        run_re, run_im = (
            tr * run_re - ti * run_im + inject[rows, :STATE_WIDTH],
            tr * run_im + ti * run_re + inject[rows, STATE_WIDTH:],
        )
        store(rows, run_re, run_im)
    last_re, last_im = last
    add = (jnp.zeros((1, STATE_WIDTH), f32), jnp.zeros((1, STATE_WIDTH), f32))
    mult = (jnp.ones((1, STATE_WIDTH), f32), jnp.zeros((1, STATE_WIDTH), f32))
    starts = []
    for sub in range(SUBS):
        starts.append((*mult, *add))
        one = slice(sub, sub + 1)
        tr, ti = last_re[one], last_im[one]
        add = (
            tr * add[0] - ti * add[1] + run_re[one],
            tr * add[1] + ti * add[0] + run_im[one],
        )
        mult = (tr * mult[0] - ti * mult[1], tr * mult[1] + ti * mult[0])
    return starts, (*mult, *add)


def inject_of(drive, in_split):
    return dot(drive, in_split[0]) + dot(drive, in_split[1])


def project_kernel(
    place,
    tokens,
    w_query,
    gain_far,
    w_key_far,
    tables_far,
    w_state_far,
    split_far,
    trans_far,
    w_value_far,
    keep,
    send,
    drive_far,
    gain,
    w_key,
    tables,
    w_state,
    in_split,
    trans,
    w_value,
    drive_near,
    arrived,
):
    far = (gain_far, w_state_far, split_far, tables_far, trans_far, w_key_far, w_value_far)
    near = (gain, w_state, in_split, tables, trans, w_key, w_value)
    copies = [
        pltpu.make_async_copy(source, target, arrived.at[i])
        for i, (source, target) in enumerate(zip(far, near))
    ]
    for copy in copies:
        copy.start()
    head = place[1]
    wide = tokens[...].astype(f32)
    scale = lax.rsqrt(jnp.mean(wide * wide, axis=-1, keepdims=True) + EPSILON)
    copies[0].wait()
    normed = (wide * scale * gain[...]).astype(bf16)

    def put(at, first, second):
        place_rows = slice(at * ROWS, (at + 1) * ROWS)
        keep[place_rows, :] = jnp.where(head == 0, first, second)
        send[place_rows, :] = jnp.where(head == 0, second, first)

    query = dot(normed, w_query[...])
    for copy in copies[1:4]:
        copy.wait()
    lane = lax.broadcasted_iota(jnp.int32, (ROWS, LANES), 1)
    first_half = lane % QK_DIM < QK_DIM // 2
    cos, sin = tables[0], tables[1]

    def turned(half):
        other = jnp.where(
            first_half,
            pltpu.roll(half, LANES - QK_DIM // 2, 1),
            pltpu.roll(half, QK_DIM // 2, 1),
        )
        return (half * cos + other * sin).astype(bf16)

    drive = dot(normed, w_state[...]).astype(bf16)
    ordered = dot(row_order(False).astype(bf16), drive).astype(bf16)
    drive_near[...] = ordered
    put(
        2,
        turned(query[:, :LANES]) * QK_DIM**-0.5,
        turned(query[:, LANES:]) * QK_DIM**-0.5,
    )
    for copy in copies[4:]:
        copy.wait()
    leaving = pltpu.make_async_copy(drive_near, drive_far, arrived.at[7])
    leaving.start()
    inject = inject_of(ordered, in_split)
    key = dot(normed, w_key[...])
    value = dot(normed, w_value[...])
    put(1, value[:, :LANES].astype(bf16), value[:, LANES:].astype(bf16))
    put(0, turned(key[:, :LANES]), turned(key[:, LANES:]))
    _, element_parts = scan_blocks(
        inject,
        trans,
        (trans[ROWS:, :STATE_WIDTH], trans[ROWS:, STATE_WIDTH:]),
        lambda where, re, im: None,
    )
    pieces = [
        member[:, tile * LANES : (tile + 1) * LANES]
        for member in element_parts
        for tile in range(STATE_WIDTH // LANES)
    ]
    element = jnp.concatenate(pieces, axis=0).astype(bf16)
    keep[3 * ROWS :, :] = element
    send[3 * ROWS :, :] = element
    leaving.wait()


def join_kernel(keep, got, out):
    for part in range(2):
        rows = slice(part * ROWS, (part + 1) * ROWS)
        out[2 * part * ROWS : (2 * part + 1) * ROWS, :] = keep[rows, :]
        out[(2 * part + 1) * ROWS : 2 * (part + 1) * ROWS, :] = got[rows, :]
    out[4 * ROWS : 4 * ROWS + EL_ROWS, :] = keep[3 * ROWS :, :]
    out[4 * ROWS + EL_ROWS :, :] = got[3 * ROWS :, :]


def attention_kernel(place, mix, sub_gain, keep, got, *rest):
    passed = rest[: RING - 1]
    out_keep, out_send, elements, scores, peak, total, numerator = rest[RING - 1 :]
    depth, head = place[0], place[1]
    pair = 2 * ROWS
    for k in range(RING - 1):
        elements[2 * EL_ROWS * k : 2 * EL_ROWS * (k + 1), :] = passed[k][2 * pair :, :]
    query = jnp.concatenate([keep[2 * ROWS : 3 * ROWS, :], got[2 * ROWS : 3 * ROWS, :]], axis=0)
    queries = (query[:, :QK_DIM], query[:, QK_DIM:])
    row = lax.broadcasted_iota(jnp.int32, (pair, pair), 0)
    column = lax.broadcasted_iota(jnp.int32, (pair, pair), 1)

    def segment(index):
        block = jnp.where(index < ROWS, head, 1 - head)
        return block * (ROWS // SEGMENT) + index % ROWS // SEGMENT

    allowed = segment(column) <= segment(row)
    own_key = jnp.concatenate([keep[:ROWS, :], got[:ROWS, :]], axis=0)
    own_value = jnp.concatenate([keep[ROWS:pair, :], got[ROWS:pair, :]], axis=0)
    for c in range(2):
        raw = dot_nt(queries[c], own_key[:, c * QK_DIM : (c + 1) * QK_DIM])
        masked = jnp.where(allowed, raw, MASK_FLOOR)
        scores[c, 0] = masked
        peak[c] = jnp.maximum(masked[:, :LANES], masked[:, LANES:])
    for k in range(1, RING):

        @pl.when(k <= depth)
        def _():
            for c in range(2):
                keys = passed[k - 1][:pair, c * QK_DIM : (c + 1) * QK_DIM]
                raw = dot_nt(queries[c], keys)
                scores[c, k] = raw
                peak[c] = jnp.maximum(peak[c], jnp.maximum(raw[:, :LANES], raw[:, LANES:]))

    tops = [jnp.max(peak[c], axis=-1, keepdims=True) for c in range(2)]
    for c in range(2):
        weight = jnp.exp(scores[c, 0] - tops[c])
        total[c] = weight[:, :LANES] + weight[:, LANES:]
        numerator[c] = dot(weight.astype(bf16), own_value)
    for k in range(1, RING):

        @pl.when(k <= depth)
        def _():
            for c in range(2):
                weight = jnp.exp(scores[c, k] - tops[c])
                total[c] += weight[:, :LANES] + weight[:, LANES:]
                numerator[c] += dot(weight.astype(bf16), passed[k - 1][pair : 2 * pair, :])

    mapped = [numerator[c] / jnp.sum(total[c], axis=-1, keepdims=True) for c in range(2)]
    difference = mapped[0] - mix[head] * mapped[1]
    mean = jnp.mean(difference * difference, axis=-1, keepdims=True)
    out = difference * lax.rsqrt(mean + EPSILON) * sub_gain[...] * (1.0 - LAMBDA_INIT)
    out_keep[...] = out[:ROWS].astype(bf16)
    out_send[...] = out[ROWS:].astype(bf16)


def state_kernel(
    place,
    init,
    got,
    elements,
    drive,
    skip,
    extra,
    decay,
    cosine,
    sine,
    in_scale,
    in_map,
    out_map,
    out,
    trans,
    product,
    in_split,
    out_split,
    states,
):
    depth, head, sequence = place[0], place[1], place[3]
    real, imag = wide_transitions(extra[...], decay[...], cosine[...], sine[...])
    put_pair(trans, ALL, real, imag)
    last = running_products(real, imag, lambda rows, re, im: put_pair(product, rows, re, im))
    scale = flat_rows(in_scale[...])
    put_split(in_split, in_map, (scale, scale))
    put_split(out_split, out_map, (1.0, -1.0))
    run_re, run_im = flat_rows(init[sequence, 0]), flat_rows(init[sequence, 1])

    def member(ref, base, index):
        tiles = STATE_WIDTH // LANES
        rows = [ref[base + index * tiles + t : base + index * tiles + t + 1, :] for t in range(tiles)]
        return jnp.concatenate(rows, axis=1).astype(f32)

    def advance(carry, ref, base, use):
        re, im = carry
        mr, mi, ar, ai = [member(ref, base, i) for i in range(4)]
        new_re, new_im = mr * re - mi * im + ar, mr * im + mi * re + ai
        return jnp.where(use, new_re, re), jnp.where(use, new_im, im)

    carry = (run_re, run_im)
    for k in range(RING - 1, 0, -1):
        use = k <= depth
        base = 2 * EL_ROWS * (k - 1)
        mine = [member(elements, base, i) for i in range(4)]
        other = [member(elements, base + EL_ROWS, i) for i in range(4)]
        early = [jnp.where(head == 0, a, b) for a, b in zip(mine, other)]
        late = [jnp.where(head == 0, b, a) for a, b in zip(mine, other)]
        for mr, mi, ar, ai in (early, late):
            re, im = carry
            new_re, new_im = mr * re - mi * im + ar, mr * im + mi * re + ai
            carry = jnp.where(use, new_re, re), jnp.where(use, new_im, im)
    carry = advance(carry, got, 3 * ROWS, head == 1)
    in_re, in_im = carry
    starts, _ = scan_blocks(
        inject_of(drive[...], in_split),
        trans,
        last,
        lambda rows, re, im: put_pair(states, rows, re, im),
    )
    add_re = jnp.concatenate([ar + mr * in_re - mi * in_im for mr, mi, ar, ai in starts], axis=0)
    add_im = jnp.concatenate([ai + mr * in_im + mi * in_re for mr, mi, ar, ai in starts], axis=0)
    for step in range(STEPS):
        rows = slice(step * SUBS, (step + 1) * SUBS)
        mr, mi = product[rows, :STATE_WIDTH], product[rows, STATE_WIDTH:]
        states[rows, :STATE_WIDTH] += mr * add_re - mi * add_im
        states[rows, STATE_WIDTH:] += mr * add_im + mi * add_re
    high, low = split_two(states[...])
    lane = lax.broadcasted_iota(jnp.int32, (GROUP, LANES), 1)
    spread = (lane % GROUP == lax.broadcasted_iota(jnp.int32, (GROUP, LANES), 0)).astype(f32)
    tiled = jnp.dot(
        skip[...], spread, precision=lax.Precision.HIGHEST, preferred_element_type=f32
    )
    own = lax.broadcasted_iota(jnp.int32, (GROUPS, LANES), 1) // GROUP
    own = own == lax.broadcasted_iota(jnp.int32, (GROUPS, LANES), 0)
    skip_row = jnp.sum(jnp.where(own, tiled, 0.0), axis=0, keepdims=True)
    mixed = (
        dot_nt(high, out_split[0])
        + dot_nt(low, out_split[0])
        + dot_nt(high, out_split[1])
        + skip_row * drive[...].astype(f32)
    )
    result = jax.nn.gelu(mixed).astype(bf16)
    out[...] = dot(row_order(True).astype(bf16), result).astype(bf16)


def output_kernel(place, state, kept, came, own, swapped_in, out, full):
    first = place[1] == 0
    mine, other = kept[...], came[...]
    acts = jnp.concatenate(
        [state[...], jnp.where(first, mine, other), jnp.where(first, other, mine)], axis=1
    )
    low_core = place[2] == 0
    for block in range(own.shape[0]):
        here, there = own[block], swapped_in[block]
        at = block % RING * 8 + block // RING
        full[at, 0] = jnp.where(low_core, here, there)
        full[at, 1] = jnp.where(low_core, there, here)
    weights = full[...].reshape(2 * own.shape[0] * own.shape[1], own.shape[2])
    out[...] = dot_nt(acts, weights).astype(bf16)


def sum_kernel(shares, out):
    total = shares[0].astype(f32)
    for i in range(1, shares.shape[0]):
        total += shares[i].astype(f32)
    out[...] = total.astype(bf16)


VMEM = pl.BlockSpec(memory_space=pltpu.VMEM)
SMEM = pl.BlockSpec(memory_space=pltpu.SMEM)
FAR = pl.BlockSpec(memory_space=pltpu.HBM)


def call(body, out_shapes, smem, args, scratch=(), far=0, far_out=0):
    near = len(args) - far
    specs = [SMEM if i in smem else VMEM if i < near else FAR for i in range(len(args))]
    return pl.pallas_call(
        body,
        out_shape=[jax.ShapeDtypeStruct(s, d) for s, d in out_shapes],
        in_specs=specs,
        out_specs=[VMEM] * (len(out_shapes) - far_out) + [FAR] * far_out,
        scratch_shapes=list(scratch),
        compiler_params=pltpu.CompilerParams(vmem_limit_bytes=20 * 1024 * 1024),
    )(*args)


def fanned(x, axis):
    shape = (lax.axis_size(axis), *x.shape)
    (copies,) = call(fan_kernel, [(shape, x.dtype)], (), (x,))
    return copies


def in_hbm(x):
    return pltpu.with_memory_space_constraint(x, pltpu.HBM)


def swapped(x, axis):
    return lax.ppermute(x, axis, [(0, 1), (1, 0)])


def local(
    tokens,
    norm_gain,
    w_query,
    w_key,
    w_value,
    w_state_in,
    decay_rate,
    rotation,
    extra_decay,
    in_map,
    out_map,
    skip_gain,
    init_state,
    mix_lambda,
    sub_gain,
    w_out_state,
    w_out_attn,
):
    depth, head, core = lax.axis_index("z"), lax.axis_index("h"), lax.axis_index("c")
    sequence = lax.axis_index("q") * 2 + core
    place = jnp.stack([depth, head, core, sequence]).astype(jnp.int32)
    gathered = lax.all_to_all(fanned(tokens, "tp"), "tp", 0, 0, tiled=True)
    weights = jnp.concatenate((w_out_state, w_out_attn), axis=0).T
    fan_weights = fanned(weights, "z")
    gathered = gathered.reshape(ROWS, tokens.shape[1])

    positions = ((depth * 2 + head) * ROWS + jnp.arange(ROWS, dtype=jnp.int32)).astype(f32)
    lane = jnp.arange(LANES, dtype=jnp.int32)
    inverse = ROTARY_BASE ** (-2.0 * (lane % (QK_DIM // 2)).astype(f32) / QK_DIM)
    angles = positions[:, None] * inverse[None, :]
    cosine_table = jnp.cos(angles)
    sine_table = jnp.where(lane % QK_DIM < QK_DIM // 2, -1.0, 1.0)[None, :] * jnp.sin(angles)
    maps = (2, GROUPS * GROUP, STATES)
    wide = ((ROWS, 2 * STATE_WIDTH), f32)
    diagonal = ((2, GROUPS * GROUP, 2 * STATE_WIDTH), bf16)
    state_params = (
        extra_decay,
        decay_rate,
        jnp.cos(rotation),
        jnp.sin(rotation),
        jnp.sqrt(-jnp.expm1(-2.0 * decay_rate)),
        jnp.swapaxes(in_map, 2, 3).reshape(maps),
    )
    tables = jnp.stack((cosine_table, sine_table))
    trans, in_split = call(
        prelude_kernel, [((ROWS + SUBS, 2 * STATE_WIDTH), f32), diagonal], (), state_params
    )

    fan_weights, gathered, trans, in_split, tables = lax.optimization_barrier(
        (fan_weights, gathered, trans, in_split, tables)
    )
    weight_rows = lax.all_to_all(fan_weights, "z", 0, 0, tiled=True)
    weight_rows = weight_rows.reshape(-1, weights.shape[1])

    payload = ((3 * ROWS + EL_ROWS, LANES), bf16)
    keep, send, drive = call(
        project_kernel,
        [payload, payload, ((ROWS, GROUPS * GROUP), bf16)],
        (0,),
        (
            place,
            gathered,
            w_query,
            in_hbm(norm_gain.reshape(1, -1)),
            in_hbm(w_key),
            in_hbm(tables),
            in_hbm(w_state_in),
            in_hbm(in_split),
            in_hbm(trans),
            in_hbm(w_value),
        ),
        [
            pltpu.VMEM((1, tokens.shape[1]), f32),
            pltpu.VMEM(w_key.shape, bf16),
            pltpu.VMEM(tables.shape, f32),
            pltpu.VMEM(w_state_in.shape, bf16),
            pltpu.VMEM(in_split.shape, bf16),
            pltpu.VMEM(trans.shape, f32),
            pltpu.VMEM(w_value.shape, bf16),
            pltpu.VMEM((ROWS, GROUPS * GROUP), bf16),
            pltpu.SemaphoreType.DMA((8,)),
        ],
        far=7,
        far_out=1,
    )
    got = swapped(send, "h")
    (shared,) = call(join_kernel, [((4 * ROWS + 2 * EL_ROWS, LANES), bf16)], (), (keep, got))

    def along(x, pairs):
        return lax.ppermute(x, "z", pairs)

    up = lambda by, first=0: [(i, i + by) for i in range(first, RING - by)]
    two = along(shared, up(2))
    six = along(shared, [(0, 6), (1, 7), (2, 0)])
    one = along(shared, up(1))
    seven = along(shared, [(0, 7)])
    four = along(two, up(2, 2))
    three = along(two, up(1, 2))
    five = along(six, [(6, 5), (7, 6), (0, 7)])
    passed = [one, two, three, four, five, six, seven]
    weight_blocks = lax.all_to_all(fanned(weight_rows, Y), Y, 0, 0, tiled=True)

    pair = (2, 2 * ROWS, LANES)
    out_keep, out_send, elements = call(
        attention_kernel,
        [((ROWS, LANES), bf16)] * 2 + [((2 * EL_ROWS * (RING - 1), LANES), bf16)],
        (0, 1),
        (place, mix_lambda, sub_gain.reshape(1, -1), keep, got, *passed),
        [pltpu.VMEM((2, RING, 2 * ROWS, 2 * ROWS), f32)] + [pltpu.VMEM(pair, f32)] * 3,
    )
    came = swapped(out_send, "h")

    (state_out,) = call(
        state_kernel,
        [((ROWS, GROUPS * GROUP), bf16)],
        (0,),
        (place, init_state, got, elements, drive, skip_gain, *state_params, out_map.reshape(maps)),
        [
            pltpu.VMEM(wide[0], f32),
            pltpu.VMEM(wide[0], f32),
            pltpu.VMEM(diagonal[0], bf16),
            pltpu.VMEM(diagonal[0], bf16),
            pltpu.VMEM(wide[0], f32),
        ],
    )

    other_blocks = swapped(weight_blocks, "c")
    width = w_out_attn.shape[1]
    blocks = (-1, width, weights.shape[1])

    (partial,) = call(
        output_kernel,
        [((ROWS, RING * 2 * 8 * width), bf16)],
        (0,),
        (
            place,
            state_out,
            out_keep,
            came,
            weight_blocks.reshape(blocks),
            other_blocks.reshape(blocks),
        ),
        [pltpu.VMEM((RING * 8, 2, width, weights.shape[1]), bf16)],
    )
    parts = partial.reshape(lax.axis_size("tp"), tokens.shape[0], -1)
    shares = lax.all_to_all(parts, "tp", 0, 0, tiled=True)
    (summed,) = call(sum_kernel, [(tokens.shape, bf16)], (), (shares,))
    return summed


def solution(mesh):
    split = Mesh(
        mesh.devices.reshape(8, 2, 4, 2, mesh.shape["tp"]), ("z", "h", "q", "c", "tp")
    )

    return jax.shard_map(
        local,
        mesh=split,
        in_specs=(
            P(SP_TP, None),
            P(),
            P(None, "tp"),
            P(None, "tp"),
            P(None, "tp"),
            P(None, "tp"),
            P("tp", None),
            P("tp", None),
            P(SP, "tp"),
            P(None, "tp", None, None),
            P(None, "tp", None, None),
            P("tp", None),
            P(None, None, "tp", None),
            P("tp"),
            P(),
            P("tp", SP),
            P("tp", SP),
        ),
        out_specs=P(SP_TP, None),
        check_vma=False,
    )
```
